512 devices in a mesh: grp: 2 (over y), sp: 32 (over z, core), tp: 8 (over x).
Axes of the slice: x: 8, y: 2, z: 16, core: 2. Of those that a mesh axis runs over, the one named last changes fastest.
The devices are a block of a 8x8x16 slice.
Arguments:
- out_gate: bfloat16 [24576, 1024], P(('grp', 'sp'), 'tp'), parts along dimension 0, may hold values from -6 to 6
- in_gate: bfloat16 [24576, 1024], P(('grp', 'sp'), 'tp'), parts along dimension 0, may hold values from -6 to 6
- conv_input: bfloat16 [24576, 1024], P(('grp', 'sp'), 'tp'), parts along dimension 0, may hold values from -6 to 6
- doc_ids: int32 [24576], P(('grp', 'sp')), parts along dimension 0, may hold values from 0 to 15, never falling along the last dimension, each value on 1 to 1536 neighbouring positions
- residual: bfloat16 [24576, 2048], P(('grp', 'sp'), 'tp'), parts along dimension 0, may hold values from -6 to 6
- conv_taps: float32 [3, 1024], P(None, 'tp'), may hold values from -6 to 6
- mix_gain: float32 [1024], P('tp'), may hold values from 0.1 to 1.9
- out_weight: bfloat16 [1024, 2048], P('tp'), may hold values from -0.1875 to 0.1875
- ffn_gain: float32 [2048], P('tp'), may hold values from 0.1 to 1.9
- routing: int32 [24576, 2], P(('grp', 'sp')), parts along dimension 0, may hold values from 0 to 63, as said below
- route_weight: float32 [24576, 2], P(('grp', 'sp')), parts along dimension 0, may hold values from 0.2 to 1.2
- expert_gate: bfloat16 [64, 2048, 512], P('sp', None, 'tp'), may hold values from -0.125 to 0.125
- expert_up: bfloat16 [64, 2048, 512], P('sp', None, 'tp'), may hold values from -0.125 to 0.125
- expert_down: bfloat16 [64, 512, 2048], P('sp', None, 'tp'), may hold values from -0.25 to 0.25
- shared_gate: bfloat16 [2048, 512], P(None, 'tp'), may hold values from -0.125 to 0.125
- shared_up: bfloat16 [2048, 512], P(None, 'tp'), may hold values from -0.125 to 0.125
- shared_down: bfloat16 [512, 2048], P(None, 'tp'), may hold values from -0.25 to 0.25
Outputs:
- layer_out: bfloat16 [24576, 2048], P(('grp', 'sp'), 'tp'), parts along dimension 0
The draws below stay inside these ranges and needn't reach their ends.
There are 2 independent parts, one for each index of `grp`. The reference program is written for one: setup_inputs(seed, part) draws one part's arguments, and reference() takes and returns one part's arrays. A program takes and returns all parts, laid end to end along the dimension named above; an argument that names none is the same for every part. Nothing has to cross between parts.
Inputs may be any that keep to these rules, and one draw needn't show every extreme that they name: `routing`: each row names 2 different experts. In each aligned block of 48 rows no expert is named by more than 3 rows, and some expert is named by exactly 3 rows. `doc_ids`: never falls along the sequence; a document holds at most 1536 positions.
All inputs are finite; a program needn't handle non-finite values.
Results may differ from the reference program's by a relative error of at most 0.017.
Values may be sent and summed in bfloat16 or wider, within the bound.
No kernel may reach another device: no remote copies, remote signals or barrier semaphores. Data moves between devices by JAX's collectives and lax.ppermute only.
A program may use at most 64 MiB of HBM per device.

```python
import math
import jax
import jax.numpy as jnp
import numpy as np
from jax import lax

D = 2048
D_CONV = 1024
E_H = 512
CONV_K = 3
TOPK = 2
EXP_DEV = 2
TOK_DEV = 384
TOKENS = 12288
EXPERTS = 64
ROWS = 48
MOST = 3
CAP_ALL = 768
DOCS = 16
DOC_MOST = 1536
N_TP = 8


def draw_conv_taps(key, part):
    key_scale = jax.random.fold_in(key, 11)
    key_taps = jax.random.fold_in(key, 12)
    scales = jnp.exp(jax.random.uniform(key_scale, (8,), jnp.float32, minval=-1.1, maxval=1.1))
    taps = jax.random.truncated_normal(key_taps, -3.0, 3.0, (CONV_K, D_CONV), jnp.float32)
    return taps * CONV_K ** (-0.5) * jnp.repeat(scales, D_CONV // 8)[None, :]


def draw_routing(key, part):
    n_dest = EXPERTS // EXP_DEV
    n_source = TOKENS // TOK_DEV
    per_source = TOK_DEV // ROWS
    n_blocks = n_source * per_source
    routes = ROWS * TOPK
    filled = routes // MOST
    dest_iota = jnp.arange(n_dest, dtype=jnp.int32)
    hot_dest = jax.random.randint(jax.random.fold_in(key, 21), (), 0, n_dest, dtype=jnp.int32)
    order_key = jax.random.fold_in(key, 22)

    def source_order(source):
        scores = jax.random.randint(jax.random.fold_in(order_key, source), (n_dest,), 0, 1 << 20, dtype=jnp.int32) * n_dest + dest_iota
        scores = jnp.where(dest_iota == hot_dest, jnp.int32(-1), scores)
        dest_order = jnp.argsort(scores).astype(jnp.int32)
        return (dest_order[:, None] * EXP_DEV + jnp.arange(EXP_DEV, dtype=jnp.int32)[None, :]).reshape(-1)
    orders = jax.vmap(source_order)(jnp.arange(n_source, dtype=jnp.int32))
    position = jnp.arange(routes, dtype=jnp.int32)
    base = filled * MOST
    which = jnp.where(position < base, position // MOST, filled + (position - base) % (EXPERTS - filled))
    listing = orders[:, which]
    listing = jnp.repeat(listing, per_source, axis=0)
    table = jnp.transpose(listing.reshape(n_blocks, TOPK, ROWS), (0, 2, 1))
    perm_key = jax.random.fold_in(key, 23)
    perms = jax.vmap(lambda block: jax.random.permutation(jax.random.fold_in(perm_key, block), ROWS).astype(jnp.int32))(jnp.arange(n_blocks, dtype=jnp.int32))
    table = jnp.take_along_axis(table, perms[:, :, None], axis=1)
    return table.reshape(TOKENS, TOPK).astype(jnp.int32)


def block_levels(stream_key, extent, cuts, least, largest):
    def one(dim, shards_of):
        heights = jax.random.uniform(jax.random.fold_in(jax.random.fold_in(stream_key, 6), dim), (shards_of,), jnp.float32, least / len(cuts), largest / len(cuts))
        return jnp.repeat(jnp.exp(heights), extent[dim] // shards_of).reshape((-1,) + (1,) * (len(extent) - dim - 1))

    gain = one(*cuts[0])
    for cut in cuts[1:]:
        gain = gain * one(*cut)
    return gain


def profile(count, total, most, lean):
    portions = [(1 << 20) // math.isqrt(grade ** lean) + 1 for grade in range(2, count + 1)]
    rest, given = total - most - (count - 1), [1] * (count - 1)
    while rest > 0:
        movable = [i for i in range(count - 1) if given[i] < most]
        mass, left = sum([portions[i] for i in movable]), rest
        for i in movable:
            extra = min(most - given[i], max(1, left * portions[i] // mass), rest)
            given[i] = given[i] + extra
            rest = rest - extra
    return np.array([most] + given)


def uneven(rng, number_of, total, limit, slope):
    if number_of == 2:
        one = jax.random.randint(rng, (), max(1, total - limit), min(limit, total - 1) + 1)
        return jnp.stack([one, total - one])
    lengths = jnp.asarray(profile(number_of, total, limit, slope), jnp.int32)
    couples = (number_of - 1) // 2
    donor, sink = lengths[1:1 + 2 * couples:2], lengths[2:2 + 2 * couples:2]
    margin = jnp.minimum(donor - 1, limit - sink)
    passed = jax.random.randint(jax.random.fold_in(rng, 1), (couples,), 0, 1 << 20) % (margin + 1)
    lengths = lengths.at[1:1 + 2 * couples:2].set(donor - passed).at[2:2 + 2 * couples:2].set(sink + passed)
    return lengths[jax.random.permutation(jax.random.fold_in(rng, 2), number_of)]


def gaussian(stream_key, extent, spread, limit, split=(), held_as=jnp.bfloat16):
    values = spread * jax.random.normal(stream_key, extent, jnp.float32)
    if split:
        values = values * block_levels(stream_key, extent, split, -0.22, 0.18)
    return jnp.clip(values, -limit, limit).astype(held_as)


def setup_inputs(seed: int = 0, part: int = 0) -> dict:
    seeds = jax.random.split(jax.random.key(seed), 18)
    own_keys = jax.random.split(jax.random.fold_in(seeds[17], part), 18)
    out_gate = gaussian(own_keys[0], (TOKENS, D_CONV), 1.0, 6.0, ((0, 32), (1, 8)))
    in_gate = gaussian(own_keys[1], (TOKENS, D_CONV), 1.0, 6.0, ((0, 32), (1, 8)))
    conv_input = gaussian(own_keys[2], (TOKENS, D_CONV), 1.0, 6.0, ((0, 32), (1, 8)))
    doc_ids = jnp.searchsorted(jnp.cumsum(uneven(own_keys[3], DOCS, TOKENS, DOC_MOST, 1)), jnp.arange(TOKENS), side="right").astype(jnp.int32)
    residual = gaussian(own_keys[4], (TOKENS, D), 1.0, 6.0, ((0, 32), (1, 8)))
    conv_taps = draw_conv_taps(jax.random.fold_in(seeds[17], 71), part)
    mix_gain = jnp.clip(1.0 + 0.18 * jax.random.normal(seeds[6], (D_CONV,), jnp.float32), 0.1, 1.9)
    out_weight = gaussian(seeds[7], (D_CONV, D), D_CONV ** -0.5, 0.1875, ((0, 8),))
    ffn_gain = jnp.clip(1.0 + 0.18 * jax.random.normal(seeds[8], (D,), jnp.float32), 0.1, 1.9)
    routing = draw_routing(jax.random.fold_in(jax.random.fold_in(seeds[17], part), 71), part)
    route_weight = jnp.clip(0.2 + 1 * jax.random.uniform(own_keys[10], (TOKENS, TOPK), jnp.float32) ** block_levels(own_keys[10], (TOKENS, TOPK), ((0, 32),), -0.2, 0.2), 0.2, 1.2)
    expert_gate = gaussian(seeds[11], (EXPERTS, D, E_H), D ** -0.5, 0.125, ((0, 32), (2, 8)))
    expert_up = gaussian(seeds[12], (EXPERTS, D, E_H), D ** -0.5, 0.125, ((0, 32), (2, 8)))
    expert_down = gaussian(seeds[13], (EXPERTS, E_H, D), E_H ** -0.5, 0.25, ((0, 32), (2, 8)))
    shared_gate = gaussian(seeds[14], (D, E_H), D ** -0.5, 0.125, ((1, 8),))
    shared_up = gaussian(seeds[15], (D, E_H), D ** -0.5, 0.125, ((1, 8),))
    shared_down = gaussian(seeds[16], (E_H, D), E_H ** -0.5, 0.25, ((1, 8),))
    return dict(out_gate=out_gate, in_gate=in_gate, conv_input=conv_input, doc_ids=doc_ids, residual=residual, conv_taps=conv_taps, mix_gain=mix_gain, out_weight=out_weight, ffn_gain=ffn_gain, routing=routing, route_weight=route_weight, expert_gate=expert_gate, expert_up=expert_up, expert_down=expert_down, shared_gate=shared_gate, shared_up=shared_up, shared_down=shared_down)


def rounded(value):
    return lax.optimization_barrier(value.astype(jnp.bfloat16)).astype(jnp.float32)

def reference(out_gate, in_gate, conv_input, doc_ids, residual, conv_taps, mix_gain, out_weight, ffn_gain, routing, route_weight, expert_gate, expert_up, expert_down, shared_gate, shared_up, shared_down):
    length = out_gate.shape[0]
    product = rounded(in_gate.astype(jnp.float32) * conv_input.astype(jnp.float32))
    extended = jnp.pad(product, ((CONV_K - 1, 0), (0, 0)))
    ext_docs = jnp.pad(doc_ids, (CONV_K - 1, 0), constant_values=-1)
    mixed = jnp.zeros(product.shape, jnp.float32)
    for k in range(CONV_K):
        keep = (ext_docs[k:k + length] == doc_ids)[:, None]
        mixed = mixed + jnp.where(keep, conv_taps[k] * extended[k:k + length], jnp.float32(0.0))
    conv_out = out_gate.astype(jnp.float32) * mixed
    scale = lax.rsqrt(lax.optimization_barrier(jnp.mean(conv_out * conv_out, axis=1, keepdims=True)) + 1e-06)
    normed = (conv_out * scale * mix_gain).astype(jnp.bfloat16)
    width = D_CONV // N_TP
    proj = jnp.zeros((length, D), jnp.float32)
    for block in range(N_TP):
        part = jnp.dot(normed[:, block * width:(block + 1) * width], out_weight[block * width:(block + 1) * width], preferred_element_type=jnp.float32)
        proj = proj + rounded(part)
    stream = (residual.astype(jnp.float32) + proj).astype(jnp.bfloat16)
    stream32 = stream.astype(jnp.float32)
    normal = (stream32 * lax.rsqrt(lax.optimization_barrier(jnp.mean(stream32 * stream32, axis=1, keepdims=True)) + 1e-06) * ffn_gain).astype(jnp.bfloat16)
    shared_hid = (jax.nn.silu(jnp.dot(normal, shared_gate, preferred_element_type=jnp.float32)) * jnp.dot(normal, shared_up, preferred_element_type=jnp.float32)).astype(jnp.bfloat16)
    shared_out = jnp.dot(shared_hid, shared_down, preferred_element_type=jnp.float32)
    padded = jnp.concatenate([normal, jnp.zeros((1, D), jnp.bfloat16)], axis=0)

    def one_expert(expert, total):
        chosen = routing == expert
        weights = lax.optimization_barrier(jnp.sum(jnp.where(chosen, route_weight, jnp.float32(0.0)), axis=1))
        weights = jnp.concatenate([weights, jnp.zeros((1,), jnp.float32)])
        index = jnp.nonzero(jnp.any(chosen, axis=1), size=CAP_ALL, fill_value=length)[0].astype(jnp.int32)
        rows = padded[index]
        gate = jnp.dot(rows, expert_gate[expert], preferred_element_type=jnp.float32)
        upper = jnp.dot(rows, expert_up[expert], preferred_element_type=jnp.float32)
        hid = (jax.nn.silu(gate) * upper).astype(jnp.bfloat16)
        result = jnp.dot(hid, expert_down[expert], preferred_element_type=jnp.float32).astype(jnp.bfloat16)
        return total.at[index].add(weights[index][:, None] * result.astype(jnp.float32))
    routed = lax.fori_loop(0, EXPERTS, one_expert, jnp.zeros((length + 1, D), jnp.float32))
    return (stream32 + shared_out + routed[:length]).astype(jnp.bfloat16)
```

```python
import jax
import jax.numpy as jnp
from jax import lax
from jax.experimental import pallas as pl
from jax.experimental.pallas import tpu as pltpu
from jax.sharding import PartitionSpec as P

CONV_K = 3
TOPK = 2
EXP_DEV = 2
LANES = 128
EPS = 1e-06


def split_bf16(value, count):
    pieces, rest = [], value
    for _ in range(count):
        piece = lax.reduce_precision(rest, 8, 7)
        pieces.append(piece)
        rest = rest - piece
    return pieces


def ring_all(shard, axis):
    n = lax.axis_size(axis)
    ahead = [(i, (i - 1) % n) for i in range(n)]
    behind = [(i, (i + 1) % n) for i in range(n)]
    got = {0: shard}
    up = down = shard
    for step in range(1, (n - 1) // 2 + 1):
        up = lax.ppermute(up, axis, ahead)
        down = lax.ppermute(down, axis, behind)
        got[step], got[n - step] = up, down
    if n % 2 == 0:
        half = shard.shape[0] // 2
        if n > 2:
            first = lax.ppermute(up[:half], axis, ahead)
            second = lax.ppermute(down[half:], axis, behind)
        else:
            first = lax.ppermute(shard[:half], axis, ahead)
            second = lax.ppermute(shard[half:], axis, behind)
        got[n // 2] = jnp.concatenate([first, second], axis=0)
    return [got[d] for d in range(n)]


def hidden_kernel(group, most, x_ref, gain_ref, w_ref, out_ref, normal_ref):
    rows = x_ref.shape[0]

    @pl.when(pl.program_id(0) == 0)
    def _():
        x = x_ref[...].astype(jnp.float32)
        mean = jnp.sum(x * x, axis=1, keepdims=True) / x.shape[1]
        normal_ref[...] = (x * lax.rsqrt(mean + EPS) * gain_ref[...]).astype(jnp.bfloat16)

    normal = normal_ref[...]
    half = w_ref.shape[1] // 2

    def shard(i):
        both = lax.dot_general(
            normal, w_ref[i], (((1,), (1,)), ((), ())), preferred_element_type=jnp.float32
        )
        gate, upper = both[:, :half], both[:, half:]
        return gate / (1.0 + jnp.exp(-gate)) * upper

    a, b = shard(0), shard(1)
    second = lax.broadcasted_iota(jnp.int32, (rows, half), 0) % group >= most
    low = lax.broadcasted_iota(jnp.int32, (rows, half), 1) < half // 2
    turned = pltpu.roll(jnp.where(second, a, b), half // 2, 1)
    kept = jnp.where(second, b, a)
    out_ref[...] = jnp.where(second == low, turned, kept).astype(jnp.bfloat16)


def hidden_of(rows, gain, weights, group, most):
    n, width = rows.shape
    shards, cols, _ = weights.shape
    return pl.pallas_call(
        lambda *refs: hidden_kernel(group, most, *refs),
        grid=(shards // 2,),
        in_specs=[
            pl.BlockSpec((n, width), lambda i: (0, 0)),
            pl.BlockSpec((1, width), lambda i: (0, 0)),
            pl.BlockSpec((2, cols, width), lambda i: (i, 0, 0)),
        ],
        out_specs=pl.BlockSpec((n, cols // 2), lambda i: (0, i)),
        out_shape=jax.ShapeDtypeStruct((n, shards // 2 * cols // 2), jnp.bfloat16),
        scratch_shapes=[pltpu.VMEM((n, width), jnp.bfloat16)],
        compiler_params=pltpu.CompilerParams(dimension_semantics=("arbitrary",)),
        name="expert_hidden",
    )(rows, gain, weights)


def down_kernel(group, most, chunk, *refs):
    pieces, (down_ref, turn_ref, out_ref, y_ref) = refs[:-4], refs[-4:]
    n = pieces[0].shape[0]
    cols = out_ref.shape[1]
    second = lax.broadcasted_iota(jnp.int32, (n, cols), 0) % group >= most
    for d, piece in enumerate(pieces):
        hid = piece[...]
        first_y = jnp.dot(hid, down_ref[0], preferred_element_type=jnp.float32)
        second_y = jnp.dot(hid, down_ref[1], preferred_element_type=jnp.float32)
        y_ref[d] = jnp.where(second, second_y, first_y).astype(jnp.bfloat16)
    turn = turn_ref[...]
    size = chunk * len(pieces)
    for g in range(n // chunk):
        mixed = y_ref[:, g * chunk : (g + 1) * chunk, :].reshape(size, cols)
        out_ref[g * size : (g + 1) * size, :] = jnp.dot(
            turn, mixed, preferred_element_type=jnp.float32
        ).astype(jnp.bfloat16)


def down_of(pieces, down, group, most):
    n = pieces[0].shape[0]
    cols = down.shape[2]
    chunk = group * 8
    size = chunk * len(pieces)
    at = jnp.arange(size, dtype=jnp.int32)
    source = at % (group * len(pieces)) // group * chunk + at // (group * len(pieces)) * group
    turn = (source[:, None] + at[:, None] % group == at[None, :]).astype(jnp.bfloat16)
    return pl.pallas_call(
        lambda *refs: down_kernel(group, most, chunk, *refs),
        out_shape=jax.ShapeDtypeStruct((n * len(pieces), cols), jnp.bfloat16),
        scratch_shapes=[pltpu.VMEM((len(pieces), n, cols), jnp.bfloat16)],
        name="expert_down",
    )(*pieces, down, turn)


def body(
    out_gate,
    in_gate,
    conv_input,
    doc_ids,
    residual,
    conv_taps,
    mix_gain,
    out_weight,
    ffn_gain,
    routing,
    route_weight,
    expert_gate,
    expert_up,
    expert_down,
    shared_gate,
    shared_up,
    shared_down,
):
    f32, bf16 = jnp.float32, jnp.bfloat16
    tokens, chans = product_shape = in_gate.shape
    width = out_weight.shape[1]
    cols = residual.shape[1]
    n_tp = lax.axis_size("tp")
    n_sp = lax.axis_size("sp")
    tp = lax.axis_index("tp")
    rows = tokens // n_tp
    experts = n_sp * EXP_DEV
    most = max(1, 2 * rows * TOPK // experts)
    group = EXP_DEV * most

    gate_t, up_t = jnp.swapaxes(expert_gate, 1, 2), jnp.swapaxes(expert_up, 1, 2)
    own_weights = jnp.concatenate([gate_t, up_t], axis=0).reshape(-1, width)
    weights = lax.all_gather(own_weights, "tp", axis=0)

    product = (in_gate.astype(f32) * conv_input.astype(f32)).astype(bf16)
    last = tokens - CONV_K + 1
    docs_row = jnp.broadcast_to(doc_ids[last:, None].astype(bf16), (CONV_K - 1, LANES))
    tail = jnp.concatenate([product[last:], docs_row], axis=1)
    before = lax.ppermute(tail, "sp", [(i, i + 1) for i in range(n_sp - 1)])
    extended = jnp.concatenate([before[:, :chans], product], axis=0).astype(f32)
    ext_docs = jnp.concatenate([before[:, chans].astype(jnp.int32), doc_ids])
    mixed = jnp.zeros(product_shape, f32)
    for k in range(CONV_K):
        keep = (ext_docs[k : k + tokens] == doc_ids)[:, None]
        mixed = mixed + jnp.where(keep, conv_taps[k] * extended[k : k + tokens], f32(0.0))
    conv_out = out_gate.astype(f32) * mixed
    partial = jnp.dot(
        (conv_out * mix_gain).astype(bf16), out_weight, preferred_element_type=f32
    ).astype(bf16)

    squares = split_bf16(jnp.sum(conv_out * conv_out, axis=1, keepdims=True), 2)
    gains = jnp.stack(split_bf16(ffn_gain, 3)).reshape(rows, -1)
    gains = jnp.broadcast_to(gains[None], (n_tp, *gains.shape)).reshape(tokens, -1)
    pad = jnp.zeros((tokens, LANES - 2 - gains.shape[1]), f32)
    extra = jnp.concatenate([gains, *squares, pad], axis=1).astype(bf16)
    sent = jnp.concatenate([partial, residual, extra], axis=1).reshape(n_tp, rows, -1)
    got = lax.all_to_all(sent, "tp", 0, 0, tiled=True)
    total = jnp.sum(got[:, :, :width].astype(f32), axis=0)
    n_gain = gains.shape[1]
    sq = jnp.sum(got[:, :, width + cols + n_gain : width + cols + n_gain + 2].astype(f32), axis=(0, 2))
    own_res = jnp.moveaxis(got[:, :, width : width + cols], 0, 1).reshape(rows, width)
    scale = lax.rsqrt(sq / (chans * n_tp) + EPS)[:, None]
    stream = (own_res.astype(f32) + total * scale).astype(bf16)
    gain = got[:, :, width + cols : width + cols + n_gain].astype(f32).reshape(n_tp, 3, cols)
    gain = ((gain[:, 0] + gain[:, 1]) + gain[:, 2]).reshape(1, width)

    mine = lax.dynamic_slice_in_dim(routing, tp * rows, rows, 0).T
    slot = jnp.arange(experts * most, dtype=jnp.int32)[:, None]
    names = (mine[0:1] == slot // most) | (mine[1:2] == slot // most)
    order = jnp.arange(rows, dtype=jnp.int32)
    ahead = (order[:, None] < order[None, :]).astype(bf16)
    earlier = jnp.dot(names.astype(bf16), ahead, preferred_element_type=f32)
    pick = (names & (earlier == (slot % most).astype(f32))).astype(bf16)
    routed = jnp.dot(pick, stream, preferred_element_type=f32).astype(bf16)
    arrived = lax.all_to_all(routed.reshape(n_sp, group, width), "sp", 0, 0, tiled=True)

    everyone = lax.all_gather(stream, "tp", axis=0, tiled=True)
    every32 = everyone.astype(f32)
    mean = jnp.sum(every32 * every32, axis=1, keepdims=True) / width
    normal = (every32 * lax.rsqrt(mean + EPS) * gain).astype(bf16)
    last_dims = (((1,), (1,)), ((), ()))
    gate = lax.dot_general(shared_gate.T, normal, last_dims, preferred_element_type=f32)
    upper = lax.dot_general(shared_up.T, normal, last_dims, preferred_element_type=f32)
    shared_hid = (jax.nn.silu(gate) * upper).astype(bf16)

    hidden = hidden_of(arrived.reshape(n_sp * group, width), gain, weights, group, most)
    pieces = ring_all(hidden, "tp")
    result = down_of(pieces, expert_down, group, most)
    returned = lax.all_to_all(result, "sp", 0, 0, tiled=True)

    wide = jnp.pad(shared_hid, ((0, 0), (0, 1024 - tokens))) if tokens < 1024 else shared_hid
    hid_all = lax.all_gather(wide, "tp", axis=0, tiled=True)[:, :tokens]
    shared_part = lax.dot_general(
        hid_all, shared_down, (((0,), (0,)), ((), ())), preferred_element_type=f32
    )

    token = jnp.arange(tokens, dtype=jnp.int32)
    all_names = (routing[:, :, None] == jnp.arange(experts, dtype=jnp.int32)).astype(bf16)
    before_it = (token[:, None] > token[None, :]) & (token[:, None] // rows == token[None, :] // rows)
    counts = jnp.dot(before_it.astype(bf16), all_names.sum(axis=1), preferred_element_type=f32)
    place = jnp.sum(counts[:, None, :] * all_names.astype(f32), axis=2).astype(jnp.int32)
    block = (token // rows - tp + n_tp) % n_tp
    entry = (
        routing // EXP_DEV * (n_tp * group)
        + block[:, None] * group
        + routing % EXP_DEV * most
        + place
    )
    at = jnp.arange(n_sp * n_tp * group, dtype=jnp.int32)[None, :]
    hits = [entry[:, k : k + 1] == at for k in range(TOPK)]
    combined = shared_part
    for weight in split_bf16(route_weight, 2):
        picks = sum(jnp.where(hits[k], weight[:, k : k + 1], f32(0.0)) for k in range(TOPK))
        combined = combined + jnp.dot(
            picks.astype(bf16), returned, preferred_element_type=f32
        )
    own = lax.dynamic_slice_in_dim(everyone, tp * cols, cols, 1)
    return (own.astype(f32) + combined).astype(bf16)


def solution(mesh):
    return jax.shard_map(
        body,
        mesh=mesh,
        in_specs=(
            P(("grp", "sp"), "tp"),
            P(("grp", "sp"), "tp"),
            P(("grp", "sp"), "tp"),
            P(("grp", "sp")),
            P(("grp", "sp"), "tp"),
            P(None, "tp"),
            P("tp"),
            P("tp", None),
            P("tp"),
            P(("grp", "sp"), None),
            P(("grp", "sp"), None),
            P("sp", None, "tp"),
            P("sp", None, "tp"),
            P("sp", None, "tp"),
            P(None, "tp"),
            P(None, "tp"),
            P(None, "tp"),
        ),
        out_specs=P(("grp", "sp"), "tp"),
        check_vma=False,
    )
```

```python
import jax
import jax.numpy as jnp
from jax import lax
from jax.experimental import pallas as pl
from jax.experimental.pallas import tpu as pltpu
from jax.sharding import PartitionSpec as P

CONV_K = 3
TOPK = 2
EXP_DEV = 2
LANES = 128
EPS = 1e-06


def split_bf16(value, count):
    pieces, rest = [], value
    for _ in range(count):
        piece = lax.reduce_precision(rest, 8, 7)
        pieces.append(piece)
        rest = rest - piece
    return pieces


def ring_all(shard, axis):
    n = lax.axis_size(axis)
    ahead = [(i, (i - 1) % n) for i in range(n)]
    behind = [(i, (i + 1) % n) for i in range(n)]
    got = {0: shard}
    up = down = shard
    for step in range(1, (n - 1) // 2 + 1):
        up = lax.ppermute(up, axis, ahead)
        down = lax.ppermute(down, axis, behind)
        got[step], got[n - step] = up, down
    if n % 2 == 0:
        half = shard.shape[0] // 2
        if n > 2:
            first = lax.ppermute(up[:half], axis, ahead)
            second = lax.ppermute(down[half:], axis, behind)
        else:
            first = lax.ppermute(shard[:half], axis, ahead)
            second = lax.ppermute(shard[half:], axis, behind)
        got[n // 2] = jnp.concatenate([first, second], axis=0)
    return [got[d] for d in range(n)]


def hidden_kernel(group, most, x_ref, gain_ref, w_ref, out_ref, normal_ref):
    rows = x_ref.shape[0]

    @pl.when(pl.program_id(0) == 0)
    def _():
        x = x_ref[...].astype(jnp.float32)
        mean = jnp.sum(x * x, axis=1, keepdims=True) / x.shape[1]
        normal_ref[...] = (x * lax.rsqrt(mean + EPS) * gain_ref[...]).astype(jnp.bfloat16)

    normal = normal_ref[...]
    half = w_ref.shape[1] // 2

    def shard(i):
        both = lax.dot_general(
            normal, w_ref[i], (((1,), (1,)), ((), ())), preferred_element_type=jnp.float32
        )
        gate, upper = both[:, :half], both[:, half:]
        return gate / (1.0 + jnp.exp(-gate)) * upper

    a, b = shard(0), shard(1)
    second = lax.broadcasted_iota(jnp.int32, (rows, half), 0) % group >= most
    low = lax.broadcasted_iota(jnp.int32, (rows, half), 1) < half // 2
    turned = pltpu.roll(jnp.where(second, a, b), half // 2, 1)
    kept = jnp.where(second, b, a)
    out_ref[...] = jnp.where(second == low, turned, kept).astype(jnp.bfloat16)


def hidden_of(rows, gain, weights, group, most):
    n, width = rows.shape
    shards, cols, _ = weights.shape
    return pl.pallas_call(
        lambda *refs: hidden_kernel(group, most, *refs),
        grid=(shards // 2,),
        in_specs=[
            pl.BlockSpec((n, width), lambda i: (0, 0)),
            pl.BlockSpec((1, width), lambda i: (0, 0)),
            pl.BlockSpec((2, cols, width), lambda i: (i, 0, 0)),
        ],
        out_specs=pl.BlockSpec((n, cols // 2), lambda i: (0, i)),
        out_shape=jax.ShapeDtypeStruct((n, shards // 2 * cols // 2), jnp.bfloat16),
        scratch_shapes=[pltpu.VMEM((n, width), jnp.bfloat16)],
        compiler_params=pltpu.CompilerParams(dimension_semantics=("arbitrary",)),
        name="expert_hidden",
    )(rows, gain, weights)


def down_kernel(group, most, chunk, *refs):
    pieces, (down_ref, turn_ref, _, out_ref, y_ref) = refs[:-5], refs[-5:]
    n = pieces[0].shape[0]
    cols = out_ref.shape[1]
    second = lax.broadcasted_iota(jnp.int32, (n, cols), 0) % group >= most
    for d, piece in enumerate(pieces):
        hid = piece[...]
        first_y = jnp.dot(hid, down_ref[0], preferred_element_type=jnp.float32)
        second_y = jnp.dot(hid, down_ref[1], preferred_element_type=jnp.float32)
        y_ref[d] = jnp.where(second, second_y, first_y).astype(jnp.bfloat16)
    turn = turn_ref[...]
    size = chunk * len(pieces)
    for g in range(n // chunk):
        mixed = y_ref[:, g * chunk : (g + 1) * chunk, :].reshape(size, cols)
        out_ref[g * size : (g + 1) * size, :] = jnp.dot(
            turn, mixed, preferred_element_type=jnp.float32
        ).astype(jnp.bfloat16)


def down_of(pieces, down, group, most, after):
    n = pieces[0].shape[0]
    cols = down.shape[2]
    chunk = group * 8
    size = chunk * len(pieces)
    at = jnp.arange(size, dtype=jnp.int32)
    source = at % (group * len(pieces)) // group * chunk + at // (group * len(pieces)) * group
    turn = (source[:, None] + at[:, None] % group == at[None, :]).astype(jnp.bfloat16)
    whole = pl.BlockSpec(memory_space=pltpu.VMEM)
    return pl.pallas_call(
        lambda *refs: down_kernel(group, most, chunk, *refs),
        in_specs=[whole] * (len(pieces) + 2) + [pl.BlockSpec(memory_space=pl.ANY)],
        out_shape=jax.ShapeDtypeStruct((n * len(pieces), cols), jnp.bfloat16),
        scratch_shapes=[pltpu.VMEM((len(pieces), n, cols), jnp.bfloat16)],
        name="expert_down",
    )(*pieces, down, turn, after)


def body(
    out_gate,
    in_gate,
    conv_input,
    doc_ids,
    residual,
    conv_taps,
    mix_gain,
    out_weight,
    ffn_gain,
    routing,
    route_weight,
    expert_gate,
    expert_up,
    expert_down,
    shared_gate,
    shared_up,
    shared_down,
):
    f32, bf16 = jnp.float32, jnp.bfloat16
    tokens, chans = product_shape = in_gate.shape
    width = out_weight.shape[1]
    cols = residual.shape[1]
    n_tp = lax.axis_size("tp")
    n_sp = lax.axis_size("sp")
    tp = lax.axis_index("tp")
    rows = tokens // n_tp
    experts = n_sp * EXP_DEV
    most = max(1, 2 * rows * TOPK // experts)
    group = EXP_DEV * most

    gate_t, up_t = jnp.swapaxes(expert_gate, 1, 2), jnp.swapaxes(expert_up, 1, 2)
    own_weights = jnp.concatenate([gate_t, up_t], axis=0).reshape(-1, width)
    weights = lax.all_gather(own_weights, "tp", axis=0)

    product = (in_gate.astype(f32) * conv_input.astype(f32)).astype(bf16)
    last = tokens - CONV_K + 1
    docs_row = jnp.broadcast_to(doc_ids[last:, None].astype(bf16), (CONV_K - 1, LANES))
    tail = jnp.concatenate([product[last:], docs_row], axis=1)
    before = lax.ppermute(tail, "sp", [(i, i + 1) for i in range(n_sp - 1)])
    extended = jnp.concatenate([before[:, :chans], product], axis=0).astype(f32)
    ext_docs = jnp.concatenate([before[:, chans].astype(jnp.int32), doc_ids])
    mixed = jnp.zeros(product_shape, f32)
    for k in range(CONV_K):
        keep = (ext_docs[k : k + tokens] == doc_ids)[:, None]
        mixed = mixed + jnp.where(keep, conv_taps[k] * extended[k : k + tokens], f32(0.0))
    conv_out = out_gate.astype(f32) * mixed
    partial = jnp.dot(
        (conv_out * mix_gain).astype(bf16), out_weight, preferred_element_type=f32
    ).astype(bf16)

    squares = split_bf16(jnp.sum(conv_out * conv_out, axis=1, keepdims=True), 2)
    gains = jnp.stack(split_bf16(ffn_gain, 3)).reshape(rows, -1)
    gains = jnp.broadcast_to(gains[None], (n_tp, *gains.shape)).reshape(tokens, -1)
    pad = jnp.zeros((tokens, LANES - 2 - gains.shape[1]), f32)
    extra = jnp.concatenate([gains, *squares, pad], axis=1).astype(bf16)
    sent = jnp.concatenate([partial, residual, extra], axis=1).reshape(n_tp, rows, -1)
    got = lax.all_to_all(sent, "tp", 0, 0, tiled=True)
    total = jnp.sum(got[:, :, :width].astype(f32), axis=0)
    n_gain = gains.shape[1]
    sq = jnp.sum(got[:, :, width + cols + n_gain : width + cols + n_gain + 2].astype(f32), axis=(0, 2))
    own_res = jnp.moveaxis(got[:, :, width : width + cols], 0, 1).reshape(rows, width)
    scale = lax.rsqrt(sq / (chans * n_tp) + EPS)[:, None]
    stream = (own_res.astype(f32) + total * scale).astype(bf16)
    gain = got[:, :, width + cols : width + cols + n_gain].astype(f32).reshape(n_tp, 3, cols)
    gain = ((gain[:, 0] + gain[:, 1]) + gain[:, 2]).reshape(1, width)

    mine = lax.dynamic_slice_in_dim(routing, tp * rows, rows, 0).T
    slot = jnp.arange(experts * most, dtype=jnp.int32)[:, None]
    names = (mine[0:1] == slot // most) | (mine[1:2] == slot // most)
    order = jnp.arange(rows, dtype=jnp.int32)
    ahead = (order[:, None] < order[None, :]).astype(bf16)
    earlier = jnp.dot(names.astype(bf16), ahead, preferred_element_type=f32)
    pick = (names & (earlier == (slot % most).astype(f32))).astype(bf16)
    routed = jnp.dot(pick, stream, preferred_element_type=f32).astype(bf16)
    arrived = lax.all_to_all(routed.reshape(n_sp, most, EXP_DEV, width), "sp", 0, 0, tiled=True)

    hidden = hidden_of(arrived.reshape(n_sp * group, width), gain, weights, group, most)
    pieces = ring_all(hidden, "tp")

    everyone = lax.all_gather(stream, "tp", axis=0, tiled=True)
    everyone, _ = lax.optimization_barrier((everyone, pieces[n_tp // 4]))
    every32 = everyone.astype(f32)
    mean = jnp.sum(every32 * every32, axis=1, keepdims=True) / width
    normal = (every32 * lax.rsqrt(mean + EPS) * gain).astype(bf16)
    last_dims = (((1,), (1,)), ((), ()))
    gate = lax.dot_general(shared_gate.T, normal, last_dims, preferred_element_type=f32)
    upper = lax.dot_general(shared_up.T, normal, last_dims, preferred_element_type=f32)
    shared_hid = (jax.nn.silu(gate) * upper).astype(bf16)

    result = down_of(pieces, expert_down, group, most, shared_hid)
    returned = lax.all_to_all(result, "sp", 0, 0, tiled=True)

    wide = jnp.pad(shared_hid, ((0, 0), (0, 1024 - tokens))) if tokens < 1024 else shared_hid
    hid_all = lax.all_gather(wide, "tp", axis=0, tiled=True)[:, :tokens]
    shared_part = lax.dot_general(
        hid_all, shared_down, (((0,), (0,)), ((), ())), preferred_element_type=f32
    )

    token = jnp.arange(tokens, dtype=jnp.int32)
    all_names = (routing[:, :, None] == jnp.arange(experts, dtype=jnp.int32)).astype(bf16)
    before_it = (token[:, None] > token[None, :]) & (token[:, None] // rows == token[None, :] // rows)
    counts = jnp.dot(before_it.astype(bf16), all_names.sum(axis=1), preferred_element_type=f32)
    place = jnp.sum(counts[:, None, :] * all_names.astype(f32), axis=2).astype(jnp.int32)
    block = (token // rows - tp + n_tp) % n_tp
    entry = (
        routing // EXP_DEV * (n_tp * group)
        + block[:, None] * group
        + routing % EXP_DEV * most
        + place
    )
    at = jnp.arange(n_sp * n_tp * group, dtype=jnp.int32)[None, :]
    hits = [entry[:, k : k + 1] == at for k in range(TOPK)]
    combined = shared_part
    for weight in split_bf16(route_weight, 2):
        picks = sum(jnp.where(hits[k], weight[:, k : k + 1], f32(0.0)) for k in range(TOPK))
        combined = combined + jnp.dot(
            picks.astype(bf16), returned, preferred_element_type=f32
        )
    own = lax.dynamic_slice_in_dim(everyone, tp * cols, cols, 1)
    return (own.astype(f32) + combined).astype(bf16)


def solution(mesh):
    return jax.shard_map(
        body,
        mesh=mesh,
        in_specs=(
            P(("grp", "sp"), "tp"),
            P(("grp", "sp"), "tp"),
            P(("grp", "sp"), "tp"),
            P(("grp", "sp")),
            P(("grp", "sp"), "tp"),
            P(None, "tp"),
            P("tp"),
            P("tp", None),
            P("tp"),
            P(("grp", "sp"), None),
            P(("grp", "sp"), None),
            P("sp", None, "tp"),
            P("sp", None, "tp"),
            P("sp", None, "tp"),
            P(None, "tp"),
            P(None, "tp"),
            P(None, "tp"),
        ),
        out_specs=P(("grp", "sp"), "tp"),
        check_vma=False,
    )
```

```python
import jax
import jax.numpy as jnp
from jax import lax
from jax.experimental import pallas as pl
from jax.experimental.pallas import tpu as pltpu
from jax.sharding import PartitionSpec as P

CONV_K = 3
TOPK = 2
EXP_DEV = 2
LANES = 128
EPS = 1e-06


def split_bf16(value, count):
    pieces, rest = [], value
    for _ in range(count):
        piece = lax.reduce_precision(rest, 8, 7)
        pieces.append(piece)
        rest = rest - piece
    return pieces


def from_further(value, axis, steps):
    n = lax.axis_size(axis)
    return lax.ppermute(value, axis, [(i, (i - steps) % n) for i in range(n)])


def gather_direct(shard, axis):
    return [shard] + [from_further(shard, axis, d) for d in range(1, lax.axis_size(axis))]


def gather_near(shard, axis):
    n = lax.axis_size(axis)
    if n != 8:
        return gather_direct(shard, axis)
    ahead2, behind2 = from_further(shard, axis, 2), from_further(shard, axis, -2)
    ahead1, behind1 = from_further(shard, axis, 1), from_further(shard, axis, -1)
    half = shard.shape[0] // 2
    over = [from_further(ahead2[:half], axis, 2), from_further(behind2[half:], axis, -2)]
    ahead3, behind3 = from_further(ahead2, axis, 1), from_further(behind2, axis, -1)
    opposite = jnp.concatenate(over, axis=0)
    return [shard, ahead1, ahead2, ahead3, opposite, behind3, behind2, behind1]


def hidden_kernel(group, most, x_ref, gain_ref, w_ref, out_ref, normal_ref):
    rows = x_ref.shape[0]

    @pl.when(pl.program_id(0) == 0)
    def _():
        x = x_ref[...].astype(jnp.float32)
        mean = jnp.sum(x * x, axis=1, keepdims=True) / x.shape[1]
        normal_ref[...] = (x * lax.rsqrt(mean + EPS) * gain_ref[...]).astype(jnp.bfloat16)

    normal = normal_ref[...]
    half = w_ref.shape[1] // 2

    def shard(i):
        both = lax.dot_general(
            normal, w_ref[i], (((1,), (1,)), ((), ())), preferred_element_type=jnp.float32
        )
        gate, upper = both[:, :half], both[:, half:]
        return gate / (1.0 + jnp.exp(-gate)) * upper

    a, b = shard(0), shard(1)
    second = lax.broadcasted_iota(jnp.int32, (rows, half), 0) % group >= most
    low = lax.broadcasted_iota(jnp.int32, (rows, half), 1) < half // 2
    turned = pltpu.roll(jnp.where(second, a, b), half // 2, 1)
    kept = jnp.where(second, b, a)
    out_ref[...] = jnp.where(second == low, turned, kept).astype(jnp.bfloat16)


def hidden_of(rows, gain, weights, group, most):
    n, width = rows.shape
    shards, cols, _ = weights.shape
    return pl.pallas_call(
        lambda *refs: hidden_kernel(group, most, *refs),
        grid=(shards // 2,),
        in_specs=[
            pl.BlockSpec((n, width), lambda i: (0, 0)),
            pl.BlockSpec((1, width), lambda i: (0, 0)),
            pl.BlockSpec((2, cols, width), lambda i: (i, 0, 0)),
        ],
        out_specs=pl.BlockSpec((n, cols // 2), lambda i: (0, i)),
        out_shape=jax.ShapeDtypeStruct((n, shards // 2 * cols // 2), jnp.bfloat16),
        scratch_shapes=[pltpu.VMEM((n, width), jnp.bfloat16)],
        compiler_params=pltpu.CompilerParams(dimension_semantics=("arbitrary",)),
        name="expert_hidden",
    )(rows, gain, weights)


def down_kernel(group, most, chunk, *refs):
    pieces, (down_ref, turn_ref, out_ref, y_ref) = refs[:-4], refs[-4:]
    n = pieces[0].shape[0]
    cols = out_ref.shape[1]
    second = lax.broadcasted_iota(jnp.int32, (n, cols), 0) % group >= most
    for d, piece in enumerate(pieces):
        hid = piece[...]
        first_y = jnp.dot(hid, down_ref[0], preferred_element_type=jnp.float32)
        second_y = jnp.dot(hid, down_ref[1], preferred_element_type=jnp.float32)
        y_ref[d] = jnp.where(second, second_y, first_y).astype(jnp.bfloat16)
    turn = turn_ref[...]
    size = chunk * len(pieces)
    for g in range(n // chunk):
        mixed = y_ref[:, g * chunk : (g + 1) * chunk, :].reshape(size, cols)
        out_ref[g * size : (g + 1) * size, :] = jnp.dot(
            turn, mixed, preferred_element_type=jnp.float32
        ).astype(jnp.bfloat16)


def down_of(pieces, down, group, most):
    n = pieces[0].shape[0]
    cols = down.shape[2]
    chunk = group * 8
    size = chunk * len(pieces)
    at = jnp.arange(size, dtype=jnp.int32)
    source = at % (group * len(pieces)) // group * chunk + at // (group * len(pieces)) * group
    turn = (source[:, None] + at[:, None] % group == at[None, :]).astype(jnp.bfloat16)
    whole = pl.BlockSpec(memory_space=pltpu.VMEM)
    return pl.pallas_call(
        lambda *refs: down_kernel(group, most, chunk, *refs),
        in_specs=[whole] * (len(pieces) + 2),
        out_shape=jax.ShapeDtypeStruct((n * len(pieces), cols), jnp.bfloat16),
        scratch_shapes=[pltpu.VMEM((len(pieces), n, cols), jnp.bfloat16)],
        name="expert_down",
    )(*pieces, down, turn)


def body(
    out_gate,
    in_gate,
    conv_input,
    doc_ids,
    residual,
    conv_taps,
    mix_gain,
    out_weight,
    ffn_gain,
    routing,
    route_weight,
    expert_gate,
    expert_up,
    expert_down,
    shared_gate,
    shared_up,
    shared_down,
):
    f32, bf16 = jnp.float32, jnp.bfloat16
    tokens, chans = product_shape = in_gate.shape
    width = out_weight.shape[1]
    cols = residual.shape[1]
    n_tp = lax.axis_size("tp")
    n_sp = lax.axis_size("sp")
    tp = lax.axis_index("tp")
    rows = tokens // n_tp
    experts = n_sp * EXP_DEV
    most = max(1, 2 * rows * TOPK // experts)
    group = EXP_DEV * most

    gate_t, up_t = jnp.swapaxes(expert_gate, 1, 2), jnp.swapaxes(expert_up, 1, 2)
    own_weights = jnp.concatenate([gate_t, up_t], axis=0).reshape(-1, width)
    weights = lax.all_gather(own_weights, "tp", axis=0)

    product = (in_gate.astype(f32) * conv_input.astype(f32)).astype(bf16)
    last = tokens - CONV_K + 1
    docs_row = jnp.broadcast_to(doc_ids[last:, None].astype(bf16), (CONV_K - 1, LANES))
    tail = jnp.concatenate([product[last:], docs_row], axis=1)
    before = lax.ppermute(tail, "sp", [(i, i + 1) for i in range(n_sp - 1)])
    extended = jnp.concatenate([before[:, :chans], product], axis=0).astype(f32)
    ext_docs = jnp.concatenate([before[:, chans].astype(jnp.int32), doc_ids])
    mixed = jnp.zeros(product_shape, f32)
    for k in range(CONV_K):
        keep = (ext_docs[k : k + tokens] == doc_ids)[:, None]
        mixed = mixed + jnp.where(keep, conv_taps[k] * extended[k : k + tokens], f32(0.0))
    conv_out = out_gate.astype(f32) * mixed
    partial = jnp.dot(
        (conv_out * mix_gain).astype(bf16), out_weight, preferred_element_type=f32
    ).astype(bf16)

    squares = split_bf16(jnp.sum(conv_out * conv_out, axis=1, keepdims=True), 2)
    gains = jnp.stack(split_bf16(ffn_gain, 3)).reshape(rows, -1)
    gains = jnp.broadcast_to(gains[None], (n_tp, *gains.shape)).reshape(tokens, -1)
    pad = jnp.zeros((tokens, LANES - 2 - gains.shape[1]), f32)
    extra = jnp.concatenate([gains, *squares, pad], axis=1).astype(bf16)
    sent = jnp.concatenate([partial, residual, extra], axis=1).reshape(n_tp, rows, -1)
    got = lax.all_to_all(sent, "tp", 0, 0, tiled=True)
    total = jnp.sum(got[:, :, :width].astype(f32), axis=0)
    n_gain = gains.shape[1]
    sq = jnp.sum(got[:, :, width + cols + n_gain : width + cols + n_gain + 2].astype(f32), axis=(0, 2))
    own_res = jnp.moveaxis(got[:, :, width : width + cols], 0, 1).reshape(rows, width)
    scale = lax.rsqrt(sq / (chans * n_tp) + EPS)[:, None]
    stream = (own_res.astype(f32) + total * scale).astype(bf16)
    gain = got[:, :, width + cols : width + cols + n_gain].astype(f32).reshape(n_tp, 3, cols)
    gain = ((gain[:, 0] + gain[:, 1]) + gain[:, 2]).reshape(1, width)

    mine = lax.dynamic_slice_in_dim(routing, tp * rows, rows, 0).T
    slot = jnp.arange(experts * most, dtype=jnp.int32)[:, None]
    names = (mine[0:1] == slot // most) | (mine[1:2] == slot // most)
    order = jnp.arange(rows, dtype=jnp.int32)
    ahead = (order[:, None] < order[None, :]).astype(bf16)
    earlier = jnp.dot(names.astype(bf16), ahead, preferred_element_type=f32)
    pick = (names & (earlier == (slot % most).astype(f32))).astype(bf16)
    routed = jnp.dot(pick, stream, preferred_element_type=f32).astype(bf16)
    arrived = lax.all_to_all(routed.reshape(n_sp, most, EXP_DEV, width), "sp", 0, 0, tiled=True)

    hidden = hidden_of(arrived.reshape(n_sp * group, width), gain, weights, group, most)
    result = down_of(gather_near(hidden, "tp"), expert_down, group, most)
    returned = lax.all_to_all(result, "sp", 0, 0, tiled=True)

    everyone = lax.all_gather(stream, "tp", axis=0, tiled=True)
    everyone, _ = lax.optimization_barrier((everyone, result))
    every32 = everyone.astype(f32)
    mean = jnp.sum(every32 * every32, axis=1, keepdims=True) / width
    normal = (every32 * lax.rsqrt(mean + EPS) * gain).astype(bf16)
    last_dims = (((1,), (1,)), ((), ()))
    gate = lax.dot_general(shared_gate.T, normal, last_dims, preferred_element_type=f32)
    upper = lax.dot_general(shared_up.T, normal, last_dims, preferred_element_type=f32)
    shared_hid = (jax.nn.silu(gate) * upper).astype(bf16)

    hid_all = jnp.concatenate(gather_direct(shared_hid, "tp"), axis=0)
    own_first = jnp.concatenate([shared_down, shared_down], axis=0)
    own_first = lax.dynamic_slice_in_dim(
        own_first, tp * shared_hid.shape[0], shared_down.shape[0], 0
    )
    shared_part = lax.dot_general(
        hid_all, own_first, (((0,), (0,)), ((), ())), preferred_element_type=f32
    )

    token = jnp.arange(tokens, dtype=jnp.int32)
    all_names = (routing[:, :, None] == jnp.arange(experts, dtype=jnp.int32)).astype(bf16)
    before_it = (token[:, None] > token[None, :]) & (token[:, None] // rows == token[None, :] // rows)
    counts = jnp.dot(before_it.astype(bf16), all_names.sum(axis=1), preferred_element_type=f32)
    place = jnp.sum(counts[:, None, :] * all_names.astype(f32), axis=2).astype(jnp.int32)
    block = (token // rows - tp + n_tp) % n_tp
    entry = (
        routing // EXP_DEV * (n_tp * group)
        + block[:, None] * group
        + routing % EXP_DEV * most
        + place
    )
    at = jnp.arange(n_sp * n_tp * group, dtype=jnp.int32)[None, :]
    hits = [entry[:, k : k + 1] == at for k in range(TOPK)]
    combined = shared_part
    for weight in split_bf16(route_weight, 2):
        picks = sum(jnp.where(hits[k], weight[:, k : k + 1], f32(0.0)) for k in range(TOPK))
        combined = combined + jnp.dot(
            picks.astype(bf16), returned, preferred_element_type=f32
        )
    own = lax.dynamic_slice_in_dim(everyone, tp * cols, cols, 1)
    return (own.astype(f32) + combined).astype(bf16)


def solution(mesh):
    return jax.shard_map(
        body,
        mesh=mesh,
        in_specs=(
            P(("grp", "sp"), "tp"),
            P(("grp", "sp"), "tp"),
            P(("grp", "sp"), "tp"),
            P(("grp", "sp")),
            P(("grp", "sp"), "tp"),
            P(None, "tp"),
            P("tp"),
            P("tp", None),
            P("tp"),
            P(("grp", "sp"), None),
            P(("grp", "sp"), None),
            P("sp", None, "tp"),
            P("sp", None, "tp"),
            P("sp", None, "tp"),
            P(None, "tp"),
            P(None, "tp"),
            P(None, "tp"),
        ),
        out_specs=P(("grp", "sp"), "tp"),
        check_vma=False,
    )
```

```python
import jax
import jax.numpy as jnp
from jax import lax
from jax.experimental import pallas as pl
from jax.experimental.pallas import tpu as pltpu
from jax.sharding import PartitionSpec as P

CONV_K = 3
TOPK = 2
EXP_DEV = 2
LANES = 128
EPS = 1e-06
GATHER_LANES = 1024


def split_bf16(value, count):
    pieces, rest = [], value
    for _ in range(count):
        piece = lax.reduce_precision(rest, 8, 7)
        pieces.append(piece)
        rest = rest - piece
    return pieces


def from_further(value, axis, steps):
    n = lax.axis_size(axis)
    return lax.ppermute(value, axis, [(i, (i - steps) % n) for i in range(n)])


def gather_direct(shard, axis):
    return [shard] + [from_further(shard, axis, d) for d in range(1, lax.axis_size(axis))]


def gather_near(shard, axis):
    n = lax.axis_size(axis)
    if n != 8:
        return gather_direct(shard, axis)
    ahead2, behind2 = from_further(shard, axis, 2), from_further(shard, axis, -2)
    ahead1, behind1 = from_further(shard, axis, 1), from_further(shard, axis, -1)
    half = shard.shape[0] // 2
    over = [from_further(ahead2[:half], axis, 2), from_further(behind2[half:], axis, -2)]
    ahead3, behind3 = from_further(ahead2, axis, 1), from_further(behind2, axis, -1)
    opposite = jnp.concatenate(over, axis=0)
    return [shard, ahead1, ahead2, ahead3, opposite, behind3, behind2, behind1]


def hidden_kernel(group, most, x_ref, gain_ref, w_ref, out_ref, normal_ref):
    rows = x_ref.shape[0]

    @pl.when(pl.program_id(0) == 0)
    def _():
        x = x_ref[...].astype(jnp.float32)
        mean = jnp.sum(x * x, axis=1, keepdims=True) / x.shape[1]
        normal_ref[...] = (x * lax.rsqrt(mean + EPS) * gain_ref[...]).astype(jnp.bfloat16)

    normal = normal_ref[...]
    half = w_ref.shape[1] // 2

    def shard(i):
        both = lax.dot_general(
            normal, w_ref[i], (((1,), (1,)), ((), ())), preferred_element_type=jnp.float32
        )
        gate, upper = both[:, :half], both[:, half:]
        return gate / (1.0 + jnp.exp(-gate)) * upper

    a, b = shard(0), shard(1)
    second = lax.broadcasted_iota(jnp.int32, (rows, half), 0) % group >= most
    low = lax.broadcasted_iota(jnp.int32, (rows, half), 1) < half // 2
    turned = pltpu.roll(jnp.where(second, a, b), half // 2, 1)
    kept = jnp.where(second, b, a)
    out_ref[...] = jnp.where(second == low, turned, kept).astype(jnp.bfloat16)


def hidden_of(rows, gain, weights, group, most):
    n, width = rows.shape
    shards, cols, _ = weights.shape
    return pl.pallas_call(
        lambda *refs: hidden_kernel(group, most, *refs),
        grid=(shards // 2,),
        in_specs=[
            pl.BlockSpec((n, width), lambda i: (0, 0)),
            pl.BlockSpec((1, width), lambda i: (0, 0)),
            pl.BlockSpec((2, cols, width), lambda i: (i, 0, 0)),
        ],
        out_specs=pl.BlockSpec((n, cols // 2), lambda i: (0, i)),
        out_shape=jax.ShapeDtypeStruct((n, shards // 2 * cols // 2), jnp.bfloat16),
        scratch_shapes=[pltpu.VMEM((n, width), jnp.bfloat16)],
        compiler_params=pltpu.CompilerParams(dimension_semantics=("arbitrary",)),
        name="expert_hidden",
    )(rows, gain, weights)


def down_kernel(group, most, chunk, *refs):
    pieces, (down_ref, turn_ref, out_ref, y_ref) = refs[:-4], refs[-4:]
    n = pieces[0].shape[0]
    cols = out_ref.shape[1]
    second = lax.broadcasted_iota(jnp.int32, (n, cols), 0) % group >= most
    for d, piece in enumerate(pieces):
        hid = piece[...]
        first_y = jnp.dot(hid, down_ref[0], preferred_element_type=jnp.float32)
        second_y = jnp.dot(hid, down_ref[1], preferred_element_type=jnp.float32)
        y_ref[d] = jnp.where(second, second_y, first_y).astype(jnp.bfloat16)
    turn = turn_ref[...]
    size = chunk * len(pieces)
    for g in range(n // chunk):
        mixed = y_ref[:, g * chunk : (g + 1) * chunk, :].reshape(size, cols)
        out_ref[g * size : (g + 1) * size, :] = jnp.dot(
            turn, mixed, preferred_element_type=jnp.float32
        ).astype(jnp.bfloat16)


def down_of(pieces, down, group, most):
    n = pieces[0].shape[0]
    cols = down.shape[2]
    chunk = group * 8
    size = chunk * len(pieces)
    at = jnp.arange(size, dtype=jnp.int32)
    source = at % (group * len(pieces)) // group * chunk + at // (group * len(pieces)) * group
    turn = (source[:, None] + at[:, None] % group == at[None, :]).astype(jnp.bfloat16)
    whole = pl.BlockSpec(memory_space=pltpu.VMEM)
    return pl.pallas_call(
        lambda *refs: down_kernel(group, most, chunk, *refs),
        in_specs=[whole] * (len(pieces) + 2),
        out_shape=jax.ShapeDtypeStruct((n * len(pieces), cols), jnp.bfloat16),
        scratch_shapes=[pltpu.VMEM((len(pieces), n, cols), jnp.bfloat16)],
        name="expert_down",
    )(*pieces, down, turn)


def body(
    out_gate,
    in_gate,
    conv_input,
    doc_ids,
    residual,
    conv_taps,
    mix_gain,
    out_weight,
    ffn_gain,
    routing,
    route_weight,
    expert_gate,
    expert_up,
    expert_down,
    shared_gate,
    shared_up,
    shared_down,
):
    f32, bf16 = jnp.float32, jnp.bfloat16
    tokens, chans = product_shape = in_gate.shape
    width = out_weight.shape[1]
    cols = residual.shape[1]
    n_tp = lax.axis_size("tp")
    n_sp = lax.axis_size("sp")
    tp = lax.axis_index("tp")
    rows = tokens // n_tp
    experts = n_sp * EXP_DEV
    most = max(1, 2 * rows * TOPK // experts)
    group = EXP_DEV * most

    gate_t, up_t = jnp.swapaxes(expert_gate, 1, 2), jnp.swapaxes(expert_up, 1, 2)
    own_weights = jnp.concatenate([gate_t, up_t], axis=0).reshape(-1, width)
    weights = lax.all_gather(own_weights, "tp", axis=0)

    product = (in_gate.astype(f32) * conv_input.astype(f32)).astype(bf16)
    last = tokens - CONV_K + 1
    docs_row = jnp.broadcast_to(doc_ids[last:, None].astype(bf16), (CONV_K - 1, LANES))
    tail = jnp.concatenate([product[last:], docs_row], axis=1)
    before = lax.ppermute(tail, "sp", [(i, i + 1) for i in range(n_sp - 1)])
    extended = jnp.concatenate([before[:, :chans], product], axis=0).astype(f32)
    ext_docs = jnp.concatenate([before[:, chans].astype(jnp.int32), doc_ids])
    mixed = jnp.zeros(product_shape, f32)
    for k in range(CONV_K):
        keep = (ext_docs[k : k + tokens] == doc_ids)[:, None]
        mixed = mixed + jnp.where(keep, conv_taps[k] * extended[k : k + tokens], f32(0.0))
    conv_out = out_gate.astype(f32) * mixed
    partial = jnp.dot(
        (conv_out * mix_gain).astype(bf16), out_weight, preferred_element_type=f32
    ).astype(bf16)

    squares = split_bf16(jnp.sum(conv_out * conv_out, axis=1, keepdims=True), 2)
    gains = jnp.stack(split_bf16(ffn_gain, 3)).reshape(rows, -1)
    gains = jnp.broadcast_to(gains[None], (n_tp, *gains.shape)).reshape(tokens, -1)
    pad = jnp.zeros((tokens, LANES - 2 - gains.shape[1]), f32)
    extra = jnp.concatenate([gains, *squares, pad], axis=1).astype(bf16)
    sent = jnp.concatenate([partial, residual, extra], axis=1).reshape(n_tp, rows, -1)
    got = lax.all_to_all(sent, "tp", 0, 0, tiled=True)
    total = jnp.sum(got[:, :, :width].astype(f32), axis=0)
    n_gain = gains.shape[1]
    sq = jnp.sum(got[:, :, width + cols + n_gain : width + cols + n_gain + 2].astype(f32), axis=(0, 2))
    own_res = jnp.moveaxis(got[:, :, width : width + cols], 0, 1).reshape(rows, width)
    scale = lax.rsqrt(sq / (chans * n_tp) + EPS)[:, None]
    stream = (own_res.astype(f32) + total * scale).astype(bf16)
    gain = got[:, :, width + cols : width + cols + n_gain].astype(f32).reshape(n_tp, 3, cols)
    gain = ((gain[:, 0] + gain[:, 1]) + gain[:, 2]).reshape(1, width)

    mine = lax.dynamic_slice_in_dim(routing, tp * rows, rows, 0).T
    slot = jnp.arange(experts * most, dtype=jnp.int32)[:, None]
    names = (mine[0:1] == slot // most) | (mine[1:2] == slot // most)
    order = jnp.arange(rows, dtype=jnp.int32)
    ahead = (order[:, None] < order[None, :]).astype(bf16)
    earlier = jnp.dot(names.astype(bf16), ahead, preferred_element_type=f32)
    pick = (names & (earlier == (slot % most).astype(f32))).astype(bf16)
    routed = jnp.dot(pick, stream, preferred_element_type=f32).astype(bf16)
    arrived = lax.all_to_all(routed.reshape(n_sp, most, EXP_DEV, width), "sp", 0, 0, tiled=True)

    hidden = hidden_of(arrived.reshape(n_sp * group, width), gain, weights, group, most)
    pieces = gather_near(hidden, "tp")
    parts = ((0, 1, 2, 6, 7), (3, 4, 5)) if n_tp == 8 else (tuple(range(n_tp)),)
    returned = []
    for part in parts:
        result = down_of([pieces[d] for d in part], expert_down, group, most)
        chunks = result.reshape(n_sp, len(part) * most, EXP_DEV, cols)
        if returned:
            chunks, _ = lax.optimization_barrier((chunks, returned[-1]))
        returned.append(lax.all_to_all(chunks, "sp", 0, 0, tiled=True).reshape(-1, cols))

    everyone = lax.all_gather(stream, "tp", axis=0, tiled=True)
    everyone, _ = lax.optimization_barrier((everyone, [pieces[d] for d in parts[-1]]))
    every32 = everyone.astype(f32)
    mean = jnp.sum(every32 * every32, axis=1, keepdims=True) / width
    normal = (every32 * lax.rsqrt(mean + EPS) * gain).astype(bf16)
    last_dims = (((1,), (1,)), ((), ()))
    gate = lax.dot_general(shared_gate.T, normal, last_dims, preferred_element_type=f32)
    upper = lax.dot_general(shared_up.T, normal, last_dims, preferred_element_type=f32)
    shared_hid = (jax.nn.silu(gate) * upper).astype(bf16)

    wide = jnp.pad(shared_hid, ((0, 0), (0, max(0, GATHER_LANES - tokens))))
    hid_all = lax.all_gather(wide, "tp", axis=0, tiled=True)[:, :tokens]
    shared_part = lax.dot_general(
        hid_all, shared_down, (((0,), (0,)), ((), ())), preferred_element_type=f32
    )

    token = jnp.arange(tokens, dtype=jnp.int32)
    all_names = (routing[:, :, None] == jnp.arange(experts, dtype=jnp.int32)).astype(bf16)
    before_it = (token[:, None] > token[None, :]) & (token[:, None] // rows == token[None, :] // rows)
    counts = jnp.dot(before_it.astype(bf16), all_names.sum(axis=1), preferred_element_type=f32)
    place = jnp.sum(counts[:, None, :] * all_names.astype(f32), axis=2).astype(jnp.int32)
    block = ((token // rows - tp + n_tp) % n_tp)[:, None]
    within = routing % EXP_DEV * most + place
    combined = shared_part
    for part, results in zip(parts, returned):
        size = len(part) * group
        number = sum(jnp.where(block == d, i, 0) for i, d in enumerate(part))
        inside = sum(jnp.where(block == d, 1, 0) for d in part) > 0
        entry = jnp.where(inside, routing // EXP_DEV * size + number * group + within, -1)
        at = jnp.arange(n_sp * size, dtype=jnp.int32)[None, :]
        hits = [entry[:, k : k + 1] == at for k in range(TOPK)]
        for weight in split_bf16(route_weight, 2):
            picks = sum(jnp.where(hits[k], weight[:, k : k + 1], f32(0.0)) for k in range(TOPK))
            combined = combined + jnp.dot(
                picks.astype(bf16), results, preferred_element_type=f32
            )
    own = lax.dynamic_slice_in_dim(everyone, tp * cols, cols, 1)
    return (own.astype(f32) + combined).astype(bf16)


def solution(mesh):
    return jax.shard_map(
        body,
        mesh=mesh,
        in_specs=(
            P(("grp", "sp"), "tp"),
            P(("grp", "sp"), "tp"),
            P(("grp", "sp"), "tp"),
            P(("grp", "sp")),
            P(("grp", "sp"), "tp"),
            P(None, "tp"),
            P("tp"),
            P("tp", None),
            P("tp"),
            P(("grp", "sp"), None),
            P(("grp", "sp"), None),
            P("sp", None, "tp"),
            P("sp", None, "tp"),
            P("sp", None, "tp"),
            P(None, "tp"),
            P(None, "tp"),
            P(None, "tp"),
        ),
        out_specs=P(("grp", "sp"), "tp"),
        check_vma=False,
    )
```

```python
import jax
import jax.numpy as jnp
from jax import lax
from jax.experimental import pallas as pl
from jax.experimental.pallas import tpu as pltpu
from jax.sharding import PartitionSpec as P

CONV_K = 3
TOPK = 2
EXP_DEV = 2
LANES = 128
EPS = 1e-06


def split_bf16(value, count):
    pieces, rest = [], value
    for _ in range(count):
        piece = lax.reduce_precision(rest, 8, 7)
        pieces.append(piece)
        rest = rest - piece
    return pieces


def from_further(value, axis, steps):
    n = lax.axis_size(axis)
    return lax.ppermute(value, axis, [(i, (i - steps) % n) for i in range(n)])


def gather_direct(shard, axis):
    return [shard] + [from_further(shard, axis, d) for d in range(1, lax.axis_size(axis))]


def gather_near(shard, axis):
    n = lax.axis_size(axis)
    if n != 8:
        return gather_direct(shard, axis)
    ahead2, behind2 = from_further(shard, axis, 2), from_further(shard, axis, -2)
    ahead1, behind1 = from_further(shard, axis, 1), from_further(shard, axis, -1)
    half = shard.shape[0] // 2
    over = [from_further(ahead2[:half], axis, 2), from_further(behind2[half:], axis, -2)]
    ahead3, behind3 = from_further(ahead2, axis, 1), from_further(behind2, axis, -1)
    opposite = jnp.concatenate(over, axis=0)
    return [shard, ahead1, ahead2, ahead3, opposite, behind3, behind2, behind1]


def hidden_kernel(group, most, x_ref, gain_ref, w_ref, out_ref, normal_ref):
    rows = x_ref.shape[0]

    @pl.when(pl.program_id(0) == 0)
    def _():
        x = x_ref[...].astype(jnp.float32)
        mean = jnp.sum(x * x, axis=1, keepdims=True) / x.shape[1]
        normal_ref[...] = (x * lax.rsqrt(mean + EPS) * gain_ref[...]).astype(jnp.bfloat16)

    normal = normal_ref[...]
    half = w_ref.shape[1] // 2

    def shard(i):
        both = lax.dot_general(
            normal, w_ref[i], (((1,), (1,)), ((), ())), preferred_element_type=jnp.float32
        )
        gate, upper = both[:, :half], both[:, half:]
        return gate / (1.0 + jnp.exp(-gate)) * upper

    a, b = shard(0), shard(1)
    second = lax.broadcasted_iota(jnp.int32, (rows, half), 0) % group >= most
    low = lax.broadcasted_iota(jnp.int32, (rows, half), 1) < half // 2
    turned = pltpu.roll(jnp.where(second, a, b), half // 2, 1)
    kept = jnp.where(second, b, a)
    out_ref[...] = jnp.where(second == low, turned, kept).astype(jnp.bfloat16)


def hidden_of(rows, gain, weights, group, most):
    n, width = rows.shape
    shards, cols, _ = weights.shape
    return pl.pallas_call(
        lambda *refs: hidden_kernel(group, most, *refs),
        grid=(shards // 2,),
        in_specs=[
            pl.BlockSpec((n, width), lambda i: (0, 0)),
            pl.BlockSpec((1, width), lambda i: (0, 0)),
            pl.BlockSpec((2, cols, width), lambda i: (i, 0, 0)),
        ],
        out_specs=pl.BlockSpec((n, cols // 2), lambda i: (0, i)),
        out_shape=jax.ShapeDtypeStruct((n, shards // 2 * cols // 2), jnp.bfloat16),
        scratch_shapes=[pltpu.VMEM((n, width), jnp.bfloat16)],
        compiler_params=pltpu.CompilerParams(dimension_semantics=("arbitrary",)),
        name="expert_hidden",
    )(rows, gain, weights)


def down_kernel(group, most, chunk, *refs):
    pieces, (down_ref, turn_ref, out_ref, y_ref) = refs[:-4], refs[-4:]
    n = pieces[0].shape[0]
    cols = out_ref.shape[1]
    second = lax.broadcasted_iota(jnp.int32, (n, cols), 0) % group >= most
    for d, piece in enumerate(pieces):
        hid = piece[...]
        first_y = jnp.dot(hid, down_ref[0], preferred_element_type=jnp.float32)
        second_y = jnp.dot(hid, down_ref[1], preferred_element_type=jnp.float32)
        y_ref[d] = jnp.where(second, second_y, first_y).astype(jnp.bfloat16)
    turn = turn_ref[...]
    size = chunk * len(pieces)
    for g in range(n // chunk):
        mixed = y_ref[:, g * chunk : (g + 1) * chunk, :].reshape(size, cols)
        out_ref[g * size : (g + 1) * size, :] = jnp.dot(
            turn, mixed, preferred_element_type=jnp.float32
        ).astype(jnp.bfloat16)


def down_of(pieces, down, group, most):
    n = pieces[0].shape[0]
    cols = down.shape[2]
    chunk = group * 8
    size = chunk * len(pieces)
    at = jnp.arange(size, dtype=jnp.int32)
    source = at % (group * len(pieces)) // group * chunk + at // (group * len(pieces)) * group
    turn = (source[:, None] + at[:, None] % group == at[None, :]).astype(jnp.bfloat16)
    whole = pl.BlockSpec(memory_space=pltpu.VMEM)
    return pl.pallas_call(
        lambda *refs: down_kernel(group, most, chunk, *refs),
        in_specs=[whole] * (len(pieces) + 2),
        out_shape=jax.ShapeDtypeStruct((n * len(pieces), cols), jnp.bfloat16),
        scratch_shapes=[pltpu.VMEM((len(pieces), n, cols), jnp.bfloat16)],
        name="expert_down",
    )(*pieces, down, turn)


def body(
    out_gate,
    in_gate,
    conv_input,
    doc_ids,
    residual,
    conv_taps,
    mix_gain,
    out_weight,
    ffn_gain,
    routing,
    route_weight,
    expert_gate,
    expert_up,
    expert_down,
    shared_gate,
    shared_up,
    shared_down,
):
    f32, bf16 = jnp.float32, jnp.bfloat16
    tokens, chans = product_shape = in_gate.shape
    width = out_weight.shape[1]
    cols = residual.shape[1]
    n_tp = lax.axis_size("tp")
    n_sp = lax.axis_size("sp")
    tp = lax.axis_index("tp")
    rows = tokens // n_tp
    experts = n_sp * EXP_DEV
    most = max(1, 2 * rows * TOPK // experts)
    group = EXP_DEV * most

    gate_t, up_t = jnp.swapaxes(expert_gate, 1, 2), jnp.swapaxes(expert_up, 1, 2)
    own_weights = jnp.concatenate([gate_t, up_t], axis=0).reshape(-1, width)
    weights = lax.all_gather(own_weights, "tp", axis=0)

    product = (in_gate.astype(f32) * conv_input.astype(f32)).astype(bf16)
    last = tokens - CONV_K + 1
    docs_row = jnp.broadcast_to(doc_ids[last:, None].astype(bf16), (CONV_K - 1, LANES))
    tail = jnp.concatenate([product[last:], docs_row], axis=1)
    before = lax.ppermute(tail, "sp", [(i, i + 1) for i in range(n_sp - 1)])
    extended = jnp.concatenate([before[:, :chans], product], axis=0).astype(f32)
    ext_docs = jnp.concatenate([before[:, chans].astype(jnp.int32), doc_ids])
    mixed = jnp.zeros(product_shape, f32)
    for k in range(CONV_K):
        keep = (ext_docs[k : k + tokens] == doc_ids)[:, None]
        mixed = mixed + jnp.where(keep, conv_taps[k] * extended[k : k + tokens], f32(0.0))
    conv_out = out_gate.astype(f32) * mixed
    conv_out = conv_out.astype(bf16)

    core = lax.axis_index("sp") % 2
    half = chans // 2
    scaled = (out_weight.astype(f32) * mix_gain[:, None]).astype(bf16)
    scaled = lax.dynamic_slice_in_dim(scaled, core * half, half, 0)
    scaled = jnp.moveaxis(scaled.reshape(half, n_tp, cols), 1, 0)
    gains = jnp.stack(split_bf16(ffn_gain, 3) + [jnp.zeros_like(ffn_gain)] * 5).astype(bf16)
    gains = jnp.broadcast_to(gains[None], (n_tp, *gains.shape))
    got = lax.all_to_all(jnp.concatenate([scaled, gains], axis=1), "tp", 0, 0, tiled=True)
    gain = got[:, half : half + 3].astype(f32)
    gain = ((gain[:, 0] + gain[:, 1]) + gain[:, 2]).reshape(1, width)
    here = got[:, :half]
    there = lax.ppermute(here, "sp", [(i, i + 1 - 2 * (i % 2)) for i in range(n_sp)])
    columns = jnp.concatenate(
        [jnp.where(core == 0, here, there), jnp.where(core == 0, there, here)], axis=1
    )

    copies = jnp.broadcast_to(conv_out[None], (n_tp, *conv_out.shape))
    channels = lax.all_to_all(copies, "tp", 0, 0, tiled=True)
    squares = jnp.sum(channels.astype(f32) * channels.astype(f32), axis=(0, 2))
    proj = lax.dot_general(
        jnp.moveaxis(channels, 0, 1).reshape(tokens, -1),
        columns.reshape(-1, cols),
        (((1,), (0,)), ((), ())),
        preferred_element_type=f32,
    )
    scale = lax.rsqrt(squares / (chans * n_tp) + EPS)[:, None]
    own = (residual.astype(f32) + proj * scale).astype(bf16)
    blocks = lax.all_to_all(own.reshape(n_tp, rows, cols), "tp", 0, 0, tiled=True)
    stream = jnp.moveaxis(blocks, 0, 1).reshape(rows, width)

    mine = lax.dynamic_slice_in_dim(routing, tp * rows, rows, 0).T
    slot = jnp.arange(experts * most, dtype=jnp.int32)[:, None]
    names = (mine[0:1] == slot // most) | (mine[1:2] == slot // most)
    order = jnp.arange(rows, dtype=jnp.int32)
    ahead = (order[:, None] < order[None, :]).astype(bf16)
    earlier = jnp.dot(names.astype(bf16), ahead, preferred_element_type=f32)
    pick = (names & (earlier == (slot % most).astype(f32))).astype(bf16)
    routed = jnp.dot(pick, stream, preferred_element_type=f32).astype(bf16)
    arrived = lax.all_to_all(routed.reshape(n_sp, most, EXP_DEV, width), "sp", 0, 0, tiled=True)

    hidden = hidden_of(arrived.reshape(n_sp * group, width), gain, weights, group, most)
    result = down_of(gather_near(hidden, "tp"), expert_down, group, most)
    returned = lax.all_to_all(result, "sp", 0, 0, tiled=True)

    everyone = lax.all_gather(stream, "tp", axis=0, tiled=True)
    everyone, _ = lax.optimization_barrier((everyone, result))
    every32 = everyone.astype(f32)
    mean = jnp.sum(every32 * every32, axis=1, keepdims=True) / width
    normal = (every32 * lax.rsqrt(mean + EPS) * gain).astype(bf16)
    last_dims = (((1,), (1,)), ((), ()))
    gate = lax.dot_general(shared_gate.T, normal, last_dims, preferred_element_type=f32)
    upper = lax.dot_general(shared_up.T, normal, last_dims, preferred_element_type=f32)
    shared_hid = (jax.nn.silu(gate) * upper).astype(bf16)

    hid_all = jnp.concatenate(gather_direct(shared_hid, "tp"), axis=0)
    own_first = jnp.concatenate([shared_down, shared_down], axis=0)
    own_first = lax.dynamic_slice_in_dim(
        own_first, tp * shared_hid.shape[0], shared_down.shape[0], 0
    )
    shared_part = lax.dot_general(
        hid_all, own_first, (((0,), (0,)), ((), ())), preferred_element_type=f32
    )

    token = jnp.arange(tokens, dtype=jnp.int32)
    all_names = (routing[:, :, None] == jnp.arange(experts, dtype=jnp.int32)).astype(bf16)
    before_it = (token[:, None] > token[None, :]) & (token[:, None] // rows == token[None, :] // rows)
    counts = jnp.dot(before_it.astype(bf16), all_names.sum(axis=1), preferred_element_type=f32)
    place = jnp.sum(counts[:, None, :] * all_names.astype(f32), axis=2).astype(jnp.int32)
    block = (token // rows - tp + n_tp) % n_tp
    entry = (
        routing // EXP_DEV * (n_tp * group)
        + block[:, None] * group
        + routing % EXP_DEV * most
        + place
    )
    at = jnp.arange(n_sp * n_tp * group, dtype=jnp.int32)[None, :]
    hits = [entry[:, k : k + 1] == at for k in range(TOPK)]
    combined = shared_part
    for weight in split_bf16(route_weight, 2):
        picks = sum(jnp.where(hits[k], weight[:, k : k + 1], f32(0.0)) for k in range(TOPK))
        combined = combined + jnp.dot(
            picks.astype(bf16), returned, preferred_element_type=f32
        )
    return (own.astype(f32) + combined).astype(bf16)


def solution(mesh):
    return jax.shard_map(
        body,
        mesh=mesh,
        in_specs=(
            P(("grp", "sp"), "tp"),
            P(("grp", "sp"), "tp"),
            P(("grp", "sp"), "tp"),
            P(("grp", "sp")),
            P(("grp", "sp"), "tp"),
            P(None, "tp"),
            P("tp"),
            P("tp", None),
            P("tp"),
            P(("grp", "sp"), None),
            P(("grp", "sp"), None),
            P("sp", None, "tp"),
            P("sp", None, "tp"),
            P("sp", None, "tp"),
            P(None, "tp"),
            P(None, "tp"),
            P(None, "tp"),
        ),
        out_specs=P(("grp", "sp"), "tp"),
        check_vma=False,
    )
```

```python
import jax
import jax.numpy as jnp
from jax import lax
from jax.experimental import pallas as pl
from jax.experimental.pallas import tpu as pltpu
from jax.sharding import PartitionSpec as P

CONV_K = 3
TOPK = 2
EXP_DEV = 2
LANES = 128
EPS = 1e-06


def split_bf16(value, count):
    pieces, rest = [], value
    for _ in range(count):
        piece = lax.reduce_precision(rest, 8, 7)
        pieces.append(piece)
        rest = rest - piece
    return pieces


def from_further(value, axis, steps):
    n = lax.axis_size(axis)
    return lax.ppermute(value, axis, [(i, (i - steps) % n) for i in range(n)])


def turned(array, start):
    twice = jnp.concatenate([array, array], axis=0)
    return lax.dynamic_slice_in_dim(twice, start, array.shape[0], 0)


def gather_direct(shard, axis):
    return [shard] + [from_further(shard, axis, d) for d in range(1, lax.axis_size(axis))]


def gather_near(shard, axis):
    n = lax.axis_size(axis)
    if n != 8:
        return gather_direct(shard, axis)
    ahead2, behind2 = from_further(shard, axis, 2), from_further(shard, axis, -2)
    ahead1, behind1 = from_further(shard, axis, 1), from_further(shard, axis, -1)
    half = shard.shape[0] // 2
    over = [from_further(ahead2[:half], axis, 2), from_further(behind2[half:], axis, -2)]
    ahead3, behind3 = from_further(ahead2, axis, 1), from_further(behind2, axis, -1)
    opposite = jnp.concatenate(over, axis=0)
    return [shard, ahead1, ahead2, ahead3, opposite, behind3, behind2, behind1]


def hidden_kernel(group, most, x_ref, gain_ref, w_ref, out_ref, normal_ref):
    rows = x_ref.shape[0]

    @pl.when(pl.program_id(0) == 0)
    def _():
        x = x_ref[...].astype(jnp.float32)
        mean = jnp.sum(x * x, axis=1, keepdims=True) / x.shape[1]
        normal_ref[...] = (x * lax.rsqrt(mean + EPS) * gain_ref[...]).astype(jnp.bfloat16)

    normal = normal_ref[...]
    half = w_ref.shape[1] // 2

    def shard(i):
        both = lax.dot_general(
            normal, w_ref[i], (((1,), (1,)), ((), ())), preferred_element_type=jnp.float32
        )
        gate, upper = both[:, :half], both[:, half:]
        return gate / (1.0 + jnp.exp(-gate)) * upper

    a, b = shard(0), shard(1)
    second = lax.broadcasted_iota(jnp.int32, (rows, half), 0) % group >= most
    low = lax.broadcasted_iota(jnp.int32, (rows, half), 1) < half // 2
    turned = pltpu.roll(jnp.where(second, a, b), half // 2, 1)
    kept = jnp.where(second, b, a)
    out_ref[...] = jnp.where(second == low, turned, kept).astype(jnp.bfloat16)


def hidden_of(rows, gain, weights, group, most):
    n, width = rows.shape
    shards, cols, _ = weights.shape
    return pl.pallas_call(
        lambda *refs: hidden_kernel(group, most, *refs),
        grid=(shards // 2,),
        in_specs=[
            pl.BlockSpec((n, width), lambda i: (0, 0)),
            pl.BlockSpec((1, width), lambda i: (0, 0)),
            pl.BlockSpec((2, cols, width), lambda i: (i, 0, 0)),
        ],
        out_specs=pl.BlockSpec((n, cols // 2), lambda i: (0, i)),
        out_shape=jax.ShapeDtypeStruct((n, shards // 2 * cols // 2), jnp.bfloat16),
        scratch_shapes=[pltpu.VMEM((n, width), jnp.bfloat16)],
        compiler_params=pltpu.CompilerParams(dimension_semantics=("arbitrary",)),
        name="expert_hidden",
    )(rows, gain, weights)


def down_kernel(group, most, chunk, *refs):
    pieces, (down_ref, turn_ref, out_ref, y_ref) = refs[:-4], refs[-4:]
    n = pieces[0].shape[0]
    cols = out_ref.shape[1]
    second = lax.broadcasted_iota(jnp.int32, (n, cols), 0) % group >= most
    for d, piece in enumerate(pieces):
        hid = piece[...]
        first_y = jnp.dot(hid, down_ref[0], preferred_element_type=jnp.float32)
        second_y = jnp.dot(hid, down_ref[1], preferred_element_type=jnp.float32)
        y_ref[d] = jnp.where(second, second_y, first_y).astype(jnp.bfloat16)
    turn = turn_ref[...]
    size = chunk * len(pieces)
    for g in range(n // chunk):
        mixed = y_ref[:, g * chunk : (g + 1) * chunk, :].reshape(size, cols)
        out_ref[g * size : (g + 1) * size, :] = jnp.dot(
            turn, mixed, preferred_element_type=jnp.float32
        ).astype(jnp.bfloat16)


def down_of(pieces, down, group, most):
    n = pieces[0].shape[0]
    cols = down.shape[2]
    chunk = group * 8
    size = chunk * len(pieces)
    at = jnp.arange(size, dtype=jnp.int32)
    source = at % (group * len(pieces)) // group * chunk + at // (group * len(pieces)) * group
    turn = (source[:, None] + at[:, None] % group == at[None, :]).astype(jnp.bfloat16)
    whole = pl.BlockSpec(memory_space=pltpu.VMEM)
    return pl.pallas_call(
        lambda *refs: down_kernel(group, most, chunk, *refs),
        in_specs=[whole] * (len(pieces) + 2),
        out_shape=jax.ShapeDtypeStruct((n * len(pieces), cols), jnp.bfloat16),
        scratch_shapes=[pltpu.VMEM((len(pieces), n, cols), jnp.bfloat16)],
        name="expert_down",
    )(*pieces, down, turn)


def body(
    out_gate,
    in_gate,
    conv_input,
    doc_ids,
    residual,
    conv_taps,
    mix_gain,
    out_weight,
    ffn_gain,
    routing,
    route_weight,
    expert_gate,
    expert_up,
    expert_down,
    shared_gate,
    shared_up,
    shared_down,
):
    f32, bf16 = jnp.float32, jnp.bfloat16
    tokens, chans = product_shape = in_gate.shape
    width = out_weight.shape[1]
    cols = residual.shape[1]
    n_tp = lax.axis_size("tp")
    n_sp = lax.axis_size("sp")
    tp = lax.axis_index("tp")
    rows = tokens // n_tp
    experts = n_sp * EXP_DEV
    most = max(1, 2 * rows * TOPK // experts)
    group = EXP_DEV * most

    gate_t, up_t = jnp.swapaxes(expert_gate, 1, 2), jnp.swapaxes(expert_up, 1, 2)
    own_weights = jnp.concatenate([gate_t, up_t], axis=0).reshape(-1, width)
    weights = lax.all_gather(own_weights, "tp", axis=0)

    product = (in_gate.astype(f32) * conv_input.astype(f32)).astype(bf16)
    last = tokens - CONV_K + 1
    docs_row = jnp.broadcast_to(doc_ids[last:, None].astype(bf16), (CONV_K - 1, LANES))
    tail = jnp.concatenate([product[last:], docs_row], axis=1)
    before = lax.ppermute(tail, "sp", [(i, i + 1) for i in range(n_sp - 1)])
    extended = jnp.concatenate([before[:, :chans], product], axis=0).astype(f32)
    ext_docs = jnp.concatenate([before[:, chans].astype(jnp.int32), doc_ids])
    mixed = jnp.zeros(product_shape, f32)
    for k in range(CONV_K):
        keep = (ext_docs[k : k + tokens] == doc_ids)[:, None]
        mixed = mixed + jnp.where(keep, conv_taps[k] * extended[k : k + tokens], f32(0.0))
    conv_out = out_gate.astype(f32) * mixed
    conv_out = conv_out.astype(bf16)

    copies = jnp.broadcast_to(conv_out[None], (n_tp, *conv_out.shape))
    channels = lax.all_to_all(copies, "tp", 0, 0, tiled=True)

    core = lax.axis_index("sp") % 2
    half = chans // 2
    scaled = (out_weight.astype(f32) * mix_gain[:, None]).astype(bf16)
    scaled = lax.dynamic_slice_in_dim(scaled, core * half, half, 0)
    scaled = jnp.moveaxis(scaled.reshape(half, n_tp, cols), 1, 0)
    gains = jnp.stack(split_bf16(ffn_gain, 3) + [jnp.zeros_like(ffn_gain)] * 5).astype(bf16)
    gains = jnp.broadcast_to(gains[None], (n_tp, *gains.shape))
    cut = turned(jnp.concatenate([scaled, gains], axis=1), tp + 1)
    cut, _ = lax.optimization_barrier((cut, copies))
    got = [cut[n_tp - 1]] + [from_further(cut[n_tp - 1 - d], "tp", d) for d in range(1, n_tp)]
    got = turned(jnp.stack(got), n_tp - tp)
    gain = got[:, half : half + 3].astype(f32)
    gain = ((gain[:, 0] + gain[:, 1]) + gain[:, 2]).reshape(1, width)
    here = got[:, :half]
    there = lax.ppermute(here, "sp", [(i, i + 1 - 2 * (i % 2)) for i in range(n_sp)])
    columns = jnp.concatenate(
        [jnp.where(core == 0, here, there), jnp.where(core == 0, there, here)], axis=1
    )

    squares = jnp.sum(channels.astype(f32) * channels.astype(f32), axis=(0, 2))
    proj = lax.dot_general(
        jnp.moveaxis(channels, 0, 1).reshape(tokens, -1),
        columns.reshape(-1, cols),
        (((1,), (0,)), ((), ())),
        preferred_element_type=f32,
    )
    scale = lax.rsqrt(squares / (chans * n_tp) + EPS)[:, None]
    own = (residual.astype(f32) + proj * scale).astype(bf16)
    blocks = lax.all_to_all(own.reshape(n_tp, rows, cols), "tp", 0, 0, tiled=True)
    stream = jnp.moveaxis(blocks, 0, 1).reshape(rows, width)

    mine = lax.dynamic_slice_in_dim(routing, tp * rows, rows, 0).T
    slot = jnp.arange(experts * most, dtype=jnp.int32)[:, None]
    names = (mine[0:1] == slot // most) | (mine[1:2] == slot // most)
    order = jnp.arange(rows, dtype=jnp.int32)
    ahead = (order[:, None] < order[None, :]).astype(bf16)
    earlier = jnp.dot(names.astype(bf16), ahead, preferred_element_type=f32)
    pick = (names & (earlier == (slot % most).astype(f32))).astype(bf16)
    routed = jnp.dot(pick, stream, preferred_element_type=f32).astype(bf16)
    arrived = lax.all_to_all(routed.reshape(n_sp, most, EXP_DEV, width), "sp", 0, 0, tiled=True)

    hidden = hidden_of(arrived.reshape(n_sp * group, width), gain, weights, group, most)
    result = down_of(gather_near(hidden, "tp"), expert_down, group, most)
    returned = lax.all_to_all(result, "sp", 0, 0, tiled=True)

    everyone = lax.all_gather(stream, "tp", axis=0, tiled=True)
    everyone, _ = lax.optimization_barrier((everyone, result))
    every32 = everyone.astype(f32)
    mean = jnp.sum(every32 * every32, axis=1, keepdims=True) / width
    normal = (every32 * lax.rsqrt(mean + EPS) * gain).astype(bf16)
    last_dims = (((1,), (1,)), ((), ()))
    gate = lax.dot_general(shared_gate.T, normal, last_dims, preferred_element_type=f32)
    upper = lax.dot_general(shared_up.T, normal, last_dims, preferred_element_type=f32)
    shared_hid = (jax.nn.silu(gate) * upper).astype(bf16)

    hid_all = jnp.concatenate(gather_direct(shared_hid, "tp"), axis=0)
    own_first = jnp.concatenate([shared_down, shared_down], axis=0)
    own_first = lax.dynamic_slice_in_dim(
        own_first, tp * shared_hid.shape[0], shared_down.shape[0], 0
    )
    shared_part = lax.dot_general(
        hid_all, own_first, (((0,), (0,)), ((), ())), preferred_element_type=f32
    )

    token = jnp.arange(tokens, dtype=jnp.int32)
    all_names = (routing[:, :, None] == jnp.arange(experts, dtype=jnp.int32)).astype(bf16)
    before_it = (token[:, None] > token[None, :]) & (token[:, None] // rows == token[None, :] // rows)
    counts = jnp.dot(before_it.astype(bf16), all_names.sum(axis=1), preferred_element_type=f32)
    place = jnp.sum(counts[:, None, :] * all_names.astype(f32), axis=2).astype(jnp.int32)
    block = (token // rows - tp + n_tp) % n_tp
    entry = (
        routing // EXP_DEV * (n_tp * group)
        + block[:, None] * group
        + routing % EXP_DEV * most
        + place
    )
    at = jnp.arange(n_sp * n_tp * group, dtype=jnp.int32)[None, :]
    hits = [entry[:, k : k + 1] == at for k in range(TOPK)]
    combined = shared_part
    for weight in split_bf16(route_weight, 2):
        picks = sum(jnp.where(hits[k], weight[:, k : k + 1], f32(0.0)) for k in range(TOPK))
        combined = combined + jnp.dot(
            picks.astype(bf16), returned, preferred_element_type=f32
        )
    return (own.astype(f32) + combined).astype(bf16)


def solution(mesh):
    return jax.shard_map(
        body,
        mesh=mesh,
        in_specs=(
            P(("grp", "sp"), "tp"),
            P(("grp", "sp"), "tp"),
            P(("grp", "sp"), "tp"),
            P(("grp", "sp")),
            P(("grp", "sp"), "tp"),
            P(None, "tp"),
            P("tp"),
            P("tp", None),
            P("tp"),
            P(("grp", "sp"), None),
            P(("grp", "sp"), None),
            P("sp", None, "tp"),
            P("sp", None, "tp"),
            P("sp", None, "tp"),
            P(None, "tp"),
            P(None, "tp"),
            P(None, "tp"),
        ),
        out_specs=P(("grp", "sp"), "tp"),
        check_vma=False,
    )
```

```python
import jax
import jax.numpy as jnp
import numpy as np
from jax import lax
from jax.experimental import pallas as pl
from jax.experimental.pallas import tpu as pltpu
from jax.sharding import PartitionSpec as P

CONV_K = 3
TOPK = 2
EXP_DEV = 2
LANES = 128
EPS = 1e-06


def split_bf16(value, count):
    pieces, rest = [], value
    for _ in range(count):
        piece = lax.reduce_precision(rest, 8, 7)
        pieces.append(piece)
        rest = rest - piece
    return pieces


def from_further(value, axis, steps):
    n = lax.axis_size(axis)
    return lax.ppermute(value, axis, [(i, (i - steps) % n) for i in range(n)])


def gather_direct(shard, axis):
    return [shard] + [from_further(shard, axis, d) for d in range(1, lax.axis_size(axis))]


def gather_near(shard, axis):
    n = lax.axis_size(axis)
    if n != 8:
        return gather_direct(shard, axis)
    ahead2, behind2 = from_further(shard, axis, 2), from_further(shard, axis, -2)
    ahead1, behind1 = from_further(shard, axis, 1), from_further(shard, axis, -1)
    half = shard.shape[0] // 2
    over = [from_further(ahead2[:half], axis, 2), from_further(behind2[half:], axis, -2)]
    ahead3, behind3 = from_further(ahead2, axis, 1), from_further(behind2, axis, -1)
    return [[p] for p in (shard, ahead1, ahead2, ahead3)] + [over] + [
        [p] for p in (behind3, behind2, behind1)
    ]


def hidden_kernel(group, most, x_ref, gain_ref, w_ref, out_ref, normal_ref):
    rows = x_ref.shape[0]

    @pl.when(pl.program_id(0) == 0)
    def _():
        x = x_ref[...].astype(jnp.float32)
        mean = jnp.sum(x * x, axis=1, keepdims=True) / x.shape[1]
        normal_ref[...] = (x * lax.rsqrt(mean + EPS) * gain_ref[...]).astype(jnp.bfloat16)

    normal = normal_ref[...]
    half = w_ref.shape[1] // 2

    def shard(i):
        both = lax.dot_general(
            normal, w_ref[i], (((1,), (1,)), ((), ())), preferred_element_type=jnp.float32
        )
        gate, upper = both[:, :half], both[:, half:]
        return gate / (1.0 + jnp.exp(-gate)) * upper

    a, b = shard(0), shard(1)
    second = lax.broadcasted_iota(jnp.int32, (rows, half), 0) % group >= most
    low = lax.broadcasted_iota(jnp.int32, (rows, half), 1) < half // 2
    turned = pltpu.roll(jnp.where(second, a, b), half // 2, 1)
    kept = jnp.where(second, b, a)
    out_ref[...] = jnp.where(second == low, turned, kept).astype(jnp.bfloat16)


def hidden_of(rows, gain, weights, group, most):
    n, width = rows.shape
    shards, cols, _ = weights.shape
    return pl.pallas_call(
        lambda *refs: hidden_kernel(group, most, *refs),
        grid=(shards // 2,),
        in_specs=[
            pl.BlockSpec((n, width), lambda i: (0, 0)),
            pl.BlockSpec((1, width), lambda i: (0, 0)),
            pl.BlockSpec((2, cols, width), lambda i: (i, 0, 0)),
        ],
        out_specs=pl.BlockSpec((n, cols // 2), lambda i: (0, i)),
        out_shape=jax.ShapeDtypeStruct((n, shards // 2 * cols // 2), jnp.bfloat16),
        scratch_shapes=[pltpu.VMEM((n, width), jnp.bfloat16)],
        compiler_params=pltpu.CompilerParams(dimension_semantics=("arbitrary",)),
        name="expert_hidden",
    )(rows, gain, weights)


def down_kernel(group, most, chunk, places, *refs):
    parts, (down_ref, turn_ref, out_ref, y_ref) = refs[:-4], refs[-4:]
    count, n, cols = y_ref.shape
    for (d, start), part in zip(places, parts):
        hid = part[...]
        size = hid.shape[0]
        second = lax.broadcasted_iota(jnp.int32, (size, cols), 0) % group >= most
        first_y = jnp.dot(hid, down_ref[0], preferred_element_type=jnp.float32)
        second_y = jnp.dot(hid, down_ref[1], preferred_element_type=jnp.float32)
        y_ref[d, start : start + size, :] = jnp.where(second, second_y, first_y).astype(
            jnp.bfloat16
        )
    turn = turn_ref[...]
    size = chunk * count
    for g in range(n // chunk):
        mixed = y_ref[:, g * chunk : (g + 1) * chunk, :].reshape(size, cols)
        out_ref[g * size : (g + 1) * size, :] = jnp.dot(
            turn, mixed, preferred_element_type=jnp.float32
        ).astype(jnp.bfloat16)


def down_of(pieces, down, group, most):
    count, n = len(pieces), sum(part.shape[0] for part in pieces[0])
    cols = down.shape[2]
    chunk = group * 8
    size = chunk * count
    at = np.arange(size)
    source = at % (group * count) // group * chunk + at // (group * count) * group
    turn = jnp.asarray(np.eye(size)[source + at % group], jnp.bfloat16)
    parts, places = [], []
    for d, piece in enumerate(pieces):
        start = 0
        for part in piece:
            parts.append(part)
            places.append((d, start))
            start += part.shape[0]
    return pl.pallas_call(
        lambda *refs: down_kernel(group, most, chunk, places, *refs),
        in_specs=[pl.BlockSpec(memory_space=pltpu.VMEM)] * (len(parts) + 2),
        out_shape=jax.ShapeDtypeStruct((n * count, cols), jnp.bfloat16),
        scratch_shapes=[pltpu.VMEM((count, n, cols), jnp.bfloat16)],
        name="expert_down",
    )(*parts, down, turn)


def body(
    out_gate,
    in_gate,
    conv_input,
    doc_ids,
    residual,
    conv_taps,
    mix_gain,
    out_weight,
    ffn_gain,
    routing,
    route_weight,
    expert_gate,
    expert_up,
    expert_down,
    shared_gate,
    shared_up,
    shared_down,
):
    f32, bf16 = jnp.float32, jnp.bfloat16
    tokens, chans = product_shape = in_gate.shape
    width = out_weight.shape[1]
    cols = residual.shape[1]
    n_tp = lax.axis_size("tp")
    n_sp = lax.axis_size("sp")
    tp = lax.axis_index("tp")
    rows = tokens // n_tp
    experts = n_sp * EXP_DEV
    most = max(1, 2 * rows * TOPK // experts)
    group = EXP_DEV * most

    gate_t, up_t = jnp.swapaxes(expert_gate, 1, 2), jnp.swapaxes(expert_up, 1, 2)
    own_weights = jnp.concatenate([gate_t, up_t], axis=0).reshape(-1, width)
    weights = lax.all_gather(own_weights, "tp", axis=0)

    product = (in_gate.astype(f32) * conv_input.astype(f32)).astype(bf16)
    last = tokens - CONV_K + 1
    docs_row = jnp.broadcast_to(doc_ids[last:, None].astype(bf16), (CONV_K - 1, LANES))
    tail = jnp.concatenate([product[last:], docs_row], axis=1)
    before = lax.ppermute(tail, "sp", [(i, i + 1) for i in range(n_sp - 1)])
    extended = jnp.concatenate([before[:, :chans], product], axis=0).astype(f32)
    ext_docs = jnp.concatenate([before[:, chans].astype(jnp.int32), doc_ids])
    mixed = jnp.zeros(product_shape, f32)
    for k in range(CONV_K):
        keep = (ext_docs[k : k + tokens] == doc_ids)[:, None]
        mixed = mixed + jnp.where(keep, conv_taps[k] * extended[k : k + tokens], f32(0.0))
    conv_out = out_gate.astype(f32) * mixed
    conv_out = conv_out.astype(bf16)

    core = lax.axis_index("sp") % 2
    half = chans // 2
    scaled = (out_weight.astype(f32) * mix_gain[:, None]).astype(bf16)
    scaled = lax.dynamic_slice_in_dim(scaled, core * half, half, 0)
    scaled = jnp.moveaxis(scaled.reshape(half, n_tp, cols), 1, 0)
    gains = jnp.stack(split_bf16(ffn_gain, 3) + [jnp.zeros_like(ffn_gain)] * 5).astype(bf16)
    gains = jnp.broadcast_to(gains[None], (n_tp, *gains.shape))
    got = lax.all_to_all(jnp.concatenate([scaled, gains], axis=1), "tp", 0, 0, tiled=True)
    gain = got[:, half : half + 3].astype(f32)
    gain = ((gain[:, 0] + gain[:, 1]) + gain[:, 2]).reshape(1, width)
    here = got[:, :half]
    there = lax.ppermute(here, "sp", [(i, i + 1 - 2 * (i % 2)) for i in range(n_sp)])
    columns = jnp.concatenate(
        [jnp.where(core == 0, here, there), jnp.where(core == 0, there, here)], axis=1
    )

    copies = jnp.broadcast_to(conv_out[None], (n_tp, *conv_out.shape))
    channels = lax.all_to_all(copies, "tp", 0, 0, tiled=True)
    squares = jnp.sum(channels.astype(f32) * channels.astype(f32), axis=(0, 2))
    proj = lax.dot_general(
        jnp.moveaxis(channels, 0, 1).reshape(tokens, -1),
        columns.reshape(-1, cols),
        (((1,), (0,)), ((), ())),
        preferred_element_type=f32,
    )
    scale = lax.rsqrt(squares / (chans * n_tp) + EPS)[:, None]
    own = (residual.astype(f32) + proj * scale).astype(bf16)
    blocks = lax.all_to_all(own.reshape(n_tp, rows, cols), "tp", 0, 0, tiled=True)
    stream = jnp.moveaxis(blocks, 0, 1).reshape(rows, width)

    mine = lax.dynamic_slice_in_dim(routing, tp * rows, rows, 0).T
    slot = jnp.arange(experts * most, dtype=jnp.int32)[:, None]
    names = (mine[0:1] == slot // most) | (mine[1:2] == slot // most)
    order = jnp.arange(rows, dtype=jnp.int32)
    ahead = (order[:, None] < order[None, :]).astype(bf16)
    earlier = jnp.dot(names.astype(bf16), ahead, preferred_element_type=f32)
    pick = (names & (earlier == (slot % most).astype(f32))).astype(bf16)
    routed = jnp.dot(pick, stream, preferred_element_type=f32).astype(bf16)
    arrived = lax.all_to_all(routed.reshape(n_sp, most, EXP_DEV, width), "sp", 0, 0, tiled=True)

    hidden = hidden_of(arrived.reshape(n_sp * group, width), gain, weights, group, most)
    result = down_of(gather_near(hidden, "tp"), expert_down, group, most)
    returned = lax.all_to_all(result, "sp", 0, 0, tiled=True)

    everyone = lax.all_gather(stream, "tp", axis=0, tiled=True)
    everyone, _ = lax.optimization_barrier((everyone, result))
    every32 = everyone.astype(f32)
    mean = jnp.sum(every32 * every32, axis=1, keepdims=True) / width
    normal = (every32 * lax.rsqrt(mean + EPS) * gain).astype(bf16)
    last_dims = (((1,), (1,)), ((), ()))
    gate = lax.dot_general(shared_gate.T, normal, last_dims, preferred_element_type=f32)
    upper = lax.dot_general(shared_up.T, normal, last_dims, preferred_element_type=f32)
    shared_hid = (jax.nn.silu(gate) * upper).astype(bf16)

    hid_all = jnp.concatenate(gather_direct(shared_hid, "tp"), axis=0)
    own_first = jnp.concatenate([shared_down, shared_down], axis=0)
    own_first = lax.dynamic_slice_in_dim(
        own_first, tp * shared_hid.shape[0], shared_down.shape[0], 0
    )
    shared_part = lax.dot_general(
        hid_all, own_first, (((0,), (0,)), ((), ())), preferred_element_type=f32
    )

    token = jnp.arange(tokens, dtype=jnp.int32)
    all_names = (routing[:, :, None] == jnp.arange(experts, dtype=jnp.int32)).astype(bf16)
    before_it = (token[:, None] > token[None, :]) & (token[:, None] // rows == token[None, :] // rows)
    counts = jnp.dot(before_it.astype(bf16), all_names.sum(axis=1), preferred_element_type=f32)
    place = jnp.sum(counts[:, None, :] * all_names.astype(f32), axis=2).astype(jnp.int32)
    block = (token // rows - tp + n_tp) % n_tp
    entry = (
        routing // EXP_DEV * (n_tp * group)
        + block[:, None] * group
        + routing % EXP_DEV * most
        + place
    )
    at = jnp.arange(n_sp * n_tp * group, dtype=jnp.int32)[None, :]
    hits = [entry[:, k : k + 1] == at for k in range(TOPK)]
    picks = sum(jnp.where(hits[k], route_weight[:, k : k + 1], f32(0.0)) for k in range(TOPK))
    combined = jnp.dot(picks.astype(bf16), returned, preferred_element_type=f32)
    shared_part = own.astype(f32) + shared_part
    return (shared_part + combined).astype(bf16)


def solution(mesh):
    return jax.shard_map(
        body,
        mesh=mesh,
        in_specs=(
            P(("grp", "sp"), "tp"),
            P(("grp", "sp"), "tp"),
            P(("grp", "sp"), "tp"),
            P(("grp", "sp")),
            P(("grp", "sp"), "tp"),
            P(None, "tp"),
            P("tp"),
            P("tp", None),
            P("tp"),
            P(("grp", "sp"), None),
            P(("grp", "sp"), None),
            P("sp", None, "tp"),
            P("sp", None, "tp"),
            P("sp", None, "tp"),
            P(None, "tp"),
            P(None, "tp"),
            P(None, "tp"),
        ),
        out_specs=P(("grp", "sp"), "tp"),
        check_vma=False,
    )
```

```python
import jax
import jax.numpy as jnp
import numpy as np
from jax import lax
from jax.experimental import pallas as pl
from jax.experimental.pallas import tpu as pltpu
from jax.sharding import PartitionSpec as P

CONV_K = 3
TOPK = 2
EXP_DEV = 2
LANES = 128
EPS = 1e-06


def split_bf16(value, count):
    pieces, rest = [], value
    for _ in range(count):
        piece = lax.reduce_precision(rest, 8, 7)
        pieces.append(piece)
        rest = rest - piece
    return pieces


def from_further(value, axis, steps):
    n = lax.axis_size(axis)
    return lax.ppermute(value, axis, [(i, (i - steps) % n) for i in range(n)])


def gather_direct(shard, axis):
    return [shard] + [from_further(shard, axis, d) for d in range(1, lax.axis_size(axis))]


def gather_ring(shard, axis):
    n = lax.axis_size(axis)
    got = {0: [shard]}
    ahead = behind = shard
    for step in range(1, (n + 1) // 2):
        ahead, behind = from_further(ahead, axis, 1), from_further(behind, axis, -1)
        got[step], got[n - step] = [ahead], [behind]
    if n % 2 == 0:
        half = shard.shape[0] // 2
        first, second = from_further(ahead[:half], axis, 1), from_further(behind[half:], axis, -1)
        got[n // 2] = [first, second]
    return [got[d] for d in range(n)]


def hidden_kernel(group, most, x_ref, gain_ref, w_ref, out_ref, normal_ref):
    rows = x_ref.shape[0]

    @pl.when(pl.program_id(0) == 0)
    def _():
        x = x_ref[...].astype(jnp.float32)
        mean = jnp.sum(x * x, axis=1, keepdims=True) / x.shape[1]
        normal_ref[...] = (x * lax.rsqrt(mean + EPS) * gain_ref[...]).astype(jnp.bfloat16)

    normal = normal_ref[...]
    half = w_ref.shape[1] // 2

    def shard(i):
        both = lax.dot_general(
            normal, w_ref[i], (((1,), (1,)), ((), ())), preferred_element_type=jnp.float32
        )
        gate, upper = both[:, :half], both[:, half:]
        return gate / (1.0 + jnp.exp(-gate)) * upper

    a, b = shard(0), shard(1)
    second = lax.broadcasted_iota(jnp.int32, (rows, half), 0) % group >= most
    low = lax.broadcasted_iota(jnp.int32, (rows, half), 1) < half // 2
    turned = pltpu.roll(jnp.where(second, a, b), half // 2, 1)
    kept = jnp.where(second, b, a)
    out_ref[...] = jnp.where(second == low, turned, kept).astype(jnp.bfloat16)


def hidden_of(rows, gain, weights, group, most):
    n, width = rows.shape
    shards, cols, _ = weights.shape
    return pl.pallas_call(
        lambda *refs: hidden_kernel(group, most, *refs),
        grid=(shards // 2,),
        in_specs=[
            pl.BlockSpec((n, width), lambda i: (0, 0)),
            pl.BlockSpec((1, width), lambda i: (0, 0)),
            pl.BlockSpec((2, cols, width), lambda i: (i, 0, 0)),
        ],
        out_specs=pl.BlockSpec((n, cols // 2), lambda i: (0, i)),
        out_shape=jax.ShapeDtypeStruct((n, shards // 2 * cols // 2), jnp.bfloat16),
        scratch_shapes=[pltpu.VMEM((n, width), jnp.bfloat16)],
        compiler_params=pltpu.CompilerParams(dimension_semantics=("arbitrary",)),
        name="expert_hidden",
    )(rows, gain, weights)


def down_kernel(group, most, chunk, places, *refs):
    parts, (down_ref, turn_ref, out_ref, y_ref) = refs[:-4], refs[-4:]
    count, n, cols = y_ref.shape
    for (d, start), part in zip(places, parts):
        hid = part[...]
        size = hid.shape[0]
        second = lax.broadcasted_iota(jnp.int32, (size, cols), 0) % group >= most
        first_y = jnp.dot(hid, down_ref[0], preferred_element_type=jnp.float32)
        second_y = jnp.dot(hid, down_ref[1], preferred_element_type=jnp.float32)
        y_ref[d, start : start + size, :] = jnp.where(second, second_y, first_y).astype(
            jnp.bfloat16
        )
    turn = turn_ref[...]
    size = chunk * count
    for g in range(n // chunk):
        mixed = y_ref[:, g * chunk : (g + 1) * chunk, :].reshape(size, cols)
        out_ref[g * size : (g + 1) * size, :] = jnp.dot(
            turn, mixed, preferred_element_type=jnp.float32
        ).astype(jnp.bfloat16)


def down_of(pieces, down, group, most):
    count, n = len(pieces), sum(part.shape[0] for part in pieces[0])
    cols = down.shape[2]
    chunk = group * 8
    size = chunk * count
    at = np.arange(size)
    source = at % (group * count) // group * chunk + at // (group * count) * group
    turn = jnp.asarray(np.eye(size)[source + at % group], jnp.bfloat16)
    parts, places = [], []
    for d, piece in enumerate(pieces):
        start = 0
        for part in piece:
            parts.append(part)
            places.append((d, start))
            start += part.shape[0]
    return pl.pallas_call(
        lambda *refs: down_kernel(group, most, chunk, places, *refs),
        in_specs=[pl.BlockSpec(memory_space=pltpu.VMEM)] * (len(parts) + 2),
        out_shape=jax.ShapeDtypeStruct((n * count, cols), jnp.bfloat16),
        scratch_shapes=[pltpu.VMEM((count, n, cols), jnp.bfloat16)],
        name="expert_down",
    )(*parts, down, turn)


def body(
    out_gate,
    in_gate,
    conv_input,
    doc_ids,
    residual,
    conv_taps,
    mix_gain,
    out_weight,
    ffn_gain,
    routing,
    route_weight,
    expert_gate,
    expert_up,
    expert_down,
    shared_gate,
    shared_up,
    shared_down,
):
    f32, bf16 = jnp.float32, jnp.bfloat16
    tokens, chans = product_shape = in_gate.shape
    width = out_weight.shape[1]
    cols = residual.shape[1]
    n_tp = lax.axis_size("tp")
    n_sp = lax.axis_size("sp")
    tp = lax.axis_index("tp")
    rows = tokens // n_tp
    experts = n_sp * EXP_DEV
    most = max(1, 2 * rows * TOPK // experts)
    group = EXP_DEV * most

    gate_t, up_t = jnp.swapaxes(expert_gate, 1, 2), jnp.swapaxes(expert_up, 1, 2)
    own_weights = jnp.concatenate([gate_t, up_t], axis=0).reshape(-1, width)
    weights = lax.all_gather(own_weights, "tp", axis=0)

    product = (in_gate.astype(f32) * conv_input.astype(f32)).astype(bf16)
    last = tokens - CONV_K + 1
    docs_row = jnp.broadcast_to(doc_ids[last:, None].astype(bf16), (CONV_K - 1, LANES))
    tail = jnp.concatenate([product[last:], docs_row], axis=1)
    before = lax.ppermute(tail, "sp", [(i, i + 1) for i in range(n_sp - 1)])
    extended = jnp.concatenate([before[:, :chans], product], axis=0).astype(f32)
    ext_docs = jnp.concatenate([before[:, chans].astype(jnp.int32), doc_ids])
    mixed = jnp.zeros(product_shape, f32)
    for k in range(CONV_K):
        keep = (ext_docs[k : k + tokens] == doc_ids)[:, None]
        mixed = mixed + jnp.where(keep, conv_taps[k] * extended[k : k + tokens], f32(0.0))
    conv_out = out_gate.astype(f32) * mixed
    conv_out = conv_out.astype(bf16)

    core = lax.axis_index("sp") % 2
    half = chans // 2
    scaled = (out_weight.astype(f32) * mix_gain[:, None]).astype(bf16)
    scaled = lax.dynamic_slice_in_dim(scaled, core * half, half, 0)
    scaled = jnp.moveaxis(scaled.reshape(half, n_tp, cols), 1, 0)
    gains = jnp.stack(split_bf16(ffn_gain, 3) + [jnp.zeros_like(ffn_gain)] * 5).astype(bf16)
    gains = jnp.broadcast_to(gains[None], (n_tp, *gains.shape))
    got = lax.all_to_all(jnp.concatenate([scaled, gains], axis=1), "tp", 0, 0, tiled=True)
    gain = got[:, half : half + 3].astype(f32)
    gain = ((gain[:, 0] + gain[:, 1]) + gain[:, 2]).reshape(1, width)
    here = got[:, :half]
    there = lax.ppermute(here, "sp", [(i, i + 1 - 2 * (i % 2)) for i in range(n_sp)])
    columns = jnp.concatenate(
        [jnp.where(core == 0, here, there), jnp.where(core == 0, there, here)], axis=1
    )

    copies = jnp.broadcast_to(conv_out[None], (n_tp, *conv_out.shape))
    channels = lax.all_to_all(copies, "tp", 0, 0, tiled=True)
    squares = jnp.sum(channels.astype(f32) * channels.astype(f32), axis=(0, 2))
    proj = lax.dot_general(
        jnp.moveaxis(channels, 0, 1).reshape(tokens, -1),
        columns.reshape(-1, cols),
        (((1,), (0,)), ((), ())),
        preferred_element_type=f32,
    )
    scale = lax.rsqrt(squares / (chans * n_tp) + EPS)[:, None]
    own = (residual.astype(f32) + proj * scale).astype(bf16)
    blocks = lax.all_to_all(own.reshape(n_tp, rows, cols), "tp", 0, 0, tiled=True)
    stream = jnp.moveaxis(blocks, 0, 1).reshape(rows, width)

    mine = lax.dynamic_slice_in_dim(routing, tp * rows, rows, 0).T
    slot = jnp.arange(experts * most, dtype=jnp.int32)[:, None]
    names = (mine[0:1] == slot // most) | (mine[1:2] == slot // most)
    order = jnp.arange(rows, dtype=jnp.int32)
    ahead = (order[:, None] < order[None, :]).astype(bf16)
    earlier = jnp.dot(names.astype(bf16), ahead, preferred_element_type=f32)
    pick = (names & (earlier == (slot % most).astype(f32))).astype(bf16)
    routed = jnp.dot(pick, stream, preferred_element_type=f32).astype(bf16)
    arrived = lax.all_to_all(routed.reshape(n_sp, most, EXP_DEV, width), "sp", 0, 0, tiled=True)

    hidden = hidden_of(arrived.reshape(n_sp * group, width), gain, weights, group, most)
    result = down_of(gather_ring(hidden, "tp"), expert_down, group, most)
    returned = lax.all_to_all(result, "sp", 0, 0, tiled=True)

    everyone = lax.all_gather(stream, "tp", axis=0, tiled=True)
    everyone, _ = lax.optimization_barrier((everyone, result))
    every32 = everyone.astype(f32)
    mean = jnp.sum(every32 * every32, axis=1, keepdims=True) / width
    normal = (every32 * lax.rsqrt(mean + EPS) * gain).astype(bf16)
    last_dims = (((1,), (1,)), ((), ()))
    gate = lax.dot_general(shared_gate.T, normal, last_dims, preferred_element_type=f32)
    upper = lax.dot_general(shared_up.T, normal, last_dims, preferred_element_type=f32)
    shared_hid = (jax.nn.silu(gate) * upper).astype(bf16)

    hid_all = jnp.concatenate(gather_direct(shared_hid, "tp"), axis=0)
    own_first = jnp.concatenate([shared_down, shared_down], axis=0)
    own_first = lax.dynamic_slice_in_dim(
        own_first, tp * shared_hid.shape[0], shared_down.shape[0], 0
    )
    shared_part = lax.dot_general(
        hid_all, own_first, (((0,), (0,)), ((), ())), preferred_element_type=f32
    )

    token = jnp.arange(tokens, dtype=jnp.int32)
    all_names = (routing[:, :, None] == jnp.arange(experts, dtype=jnp.int32)).astype(bf16)
    before_it = (token[:, None] > token[None, :]) & (token[:, None] // rows == token[None, :] // rows)
    counts = jnp.dot(before_it.astype(bf16), all_names.sum(axis=1), preferred_element_type=f32)
    place = jnp.sum(counts[:, None, :] * all_names.astype(f32), axis=2).astype(jnp.int32)
    block = (token // rows - tp + n_tp) % n_tp
    entry = (
        routing // EXP_DEV * (n_tp * group)
        + block[:, None] * group
        + routing % EXP_DEV * most
        + place
    )
    at = jnp.arange(n_sp * n_tp * group, dtype=jnp.int32)[None, :]
    hits = [entry[:, k : k + 1] == at for k in range(TOPK)]
    picks = sum(jnp.where(hits[k], route_weight[:, k : k + 1], f32(0.0)) for k in range(TOPK))
    combined = jnp.dot(picks.astype(bf16), returned, preferred_element_type=f32)
    shared_part = own.astype(f32) + shared_part
    return (shared_part + combined).astype(bf16)


def solution(mesh):
    return jax.shard_map(
        body,
        mesh=mesh,
        in_specs=(
            P(("grp", "sp"), "tp"),
            P(("grp", "sp"), "tp"),
            P(("grp", "sp"), "tp"),
            P(("grp", "sp")),
            P(("grp", "sp"), "tp"),
            P(None, "tp"),
            P("tp"),
            P("tp", None),
            P("tp"),
            P(("grp", "sp"), None),
            P(("grp", "sp"), None),
            P("sp", None, "tp"),
            P("sp", None, "tp"),
            P("sp", None, "tp"),
            P(None, "tp"),
            P(None, "tp"),
            P(None, "tp"),
        ),
        out_specs=P(("grp", "sp"), "tp"),
        check_vma=False,
    )
```

```python
import jax
import jax.numpy as jnp
import numpy as np
from jax import lax
from jax.experimental import pallas as pl
from jax.experimental.pallas import tpu as pltpu
from jax.sharding import PartitionSpec as P

CONV_K = 3
TOPK = 2
EXP_DEV = 2
LANES = 128
EPS = 1e-06


def split_bf16(value, count):
    pieces, rest = [], value
    for _ in range(count):
        piece = lax.reduce_precision(rest, 8, 7)
        pieces.append(piece)
        rest = rest - piece
    return pieces


def from_further(value, axis, steps):
    n = lax.axis_size(axis)
    return lax.ppermute(value, axis, [(i, (i - steps) % n) for i in range(n)])


def gather_direct(shard, axis):
    return [shard] + [from_further(shard, axis, d) for d in range(1, lax.axis_size(axis))]


def gather_near(shard, axis):
    n = lax.axis_size(axis)
    if n != 8:
        return gather_direct(shard, axis)
    ahead2, behind2 = from_further(shard, axis, 2), from_further(shard, axis, -2)
    ahead1, behind1 = from_further(shard, axis, 1), from_further(shard, axis, -1)
    half = shard.shape[0] // 2
    over = [from_further(ahead2[:half], axis, 2), from_further(behind2[half:], axis, -2)]
    ahead3, behind3 = from_further(ahead2, axis, 1), from_further(behind2, axis, -1)
    return [[p] for p in (shard, ahead1, ahead2, ahead3)] + [over] + [
        [p] for p in (behind3, behind2, behind1)
    ]


def hidden_kernel(group, most, x_ref, gain_ref, w_ref, out_ref, normal_ref):
    rows = x_ref.shape[0]

    @pl.when(pl.program_id(0) == 0)
    def _():
        x = x_ref[...].astype(jnp.float32)
        mean = jnp.sum(x * x, axis=1, keepdims=True) / x.shape[1]
        normal_ref[...] = (x * lax.rsqrt(mean + EPS) * gain_ref[...]).astype(jnp.bfloat16)

    normal = normal_ref[...]
    half = w_ref.shape[1] // 2

    def shard(i):
        both = lax.dot_general(
            normal, w_ref[i], (((1,), (1,)), ((), ())), preferred_element_type=jnp.float32
        )
        gate, upper = both[:, :half], both[:, half:]
        return gate / (1.0 + jnp.exp(-gate)) * upper

    a, b = shard(0), shard(1)
    second = lax.broadcasted_iota(jnp.int32, (rows, half), 0) % group >= most
    low = lax.broadcasted_iota(jnp.int32, (rows, half), 1) < half // 2
    turned = pltpu.roll(jnp.where(second, a, b), half // 2, 1)
    kept = jnp.where(second, b, a)
    out_ref[...] = jnp.where(second == low, turned, kept).astype(jnp.bfloat16)


def hidden_of(rows, gain, weights, group, most):
    n, width = rows.shape
    shards, cols, _ = weights.shape
    return pl.pallas_call(
        lambda *refs: hidden_kernel(group, most, *refs),
        grid=(shards // 2,),
        in_specs=[
            pl.BlockSpec((n, width), lambda i: (0, 0)),
            pl.BlockSpec((1, width), lambda i: (0, 0)),
            pl.BlockSpec((2, cols, width), lambda i: (i, 0, 0)),
        ],
        out_specs=pl.BlockSpec((n, cols // 2), lambda i: (0, i)),
        out_shape=jax.ShapeDtypeStruct((n, shards // 2 * cols // 2), jnp.bfloat16),
        scratch_shapes=[pltpu.VMEM((n, width), jnp.bfloat16)],
        compiler_params=pltpu.CompilerParams(dimension_semantics=("arbitrary",)),
        name="expert_hidden",
    )(rows, gain, weights)


def down_kernel(group, most, chunk, places, *refs):
    parts, (down_ref, turn_ref, out_ref, y_ref) = refs[:-4], refs[-4:]
    count, n, cols = y_ref.shape
    for (d, start), part in zip(places, parts):
        hid = part[...]
        size = hid.shape[0]
        second = lax.broadcasted_iota(jnp.int32, (size, cols), 0) % group >= most
        both = jnp.dot(hid, down_ref[...], preferred_element_type=jnp.float32)
        first_y, second_y = both[:, :cols], both[:, cols:]
        y_ref[d, start : start + size, :] = jnp.where(second, second_y, first_y).astype(
            jnp.bfloat16
        )
    turn = turn_ref[...]
    size = chunk * count
    for g in range(n // chunk):
        mixed = y_ref[:, g * chunk : (g + 1) * chunk, :].reshape(size, cols)
        out_ref[g * size : (g + 1) * size, :] = jnp.dot(
            turn, mixed, preferred_element_type=jnp.float32
        ).astype(jnp.bfloat16)


def down_of(pieces, down, group, most):
    count, n = len(pieces), sum(part.shape[0] for part in pieces[0])
    cols = down.shape[2]
    chunk = group * 8
    size = chunk * count
    at = np.arange(size)
    source = at % (group * count) // group * chunk + at // (group * count) * group
    turn = jnp.asarray(np.eye(size)[source + at % group], jnp.bfloat16)
    parts, places = [], []
    for d, piece in enumerate(pieces):
        start = 0
        for part in piece:
            parts.append(part)
            places.append((d, start))
            start += part.shape[0]
    return pl.pallas_call(
        lambda *refs: down_kernel(group, most, chunk, places, *refs),
        in_specs=[pl.BlockSpec(memory_space=pltpu.VMEM)] * (len(parts) + 2),
        out_shape=jax.ShapeDtypeStruct((n * count, cols), jnp.bfloat16),
        scratch_shapes=[pltpu.VMEM((count, n, cols), jnp.bfloat16)],
        name="expert_down",
    )(*parts, jnp.concatenate([down[0], down[1]], axis=1), turn)


def body(
    out_gate,
    in_gate,
    conv_input,
    doc_ids,
    residual,
    conv_taps,
    mix_gain,
    out_weight,
    ffn_gain,
    routing,
    route_weight,
    expert_gate,
    expert_up,
    expert_down,
    shared_gate,
    shared_up,
    shared_down,
):
    f32, bf16 = jnp.float32, jnp.bfloat16
    tokens, chans = product_shape = in_gate.shape
    width = out_weight.shape[1]
    cols = residual.shape[1]
    n_tp = lax.axis_size("tp")
    n_sp = lax.axis_size("sp")
    tp = lax.axis_index("tp")
    rows = tokens // n_tp
    experts = n_sp * EXP_DEV
    most = max(1, 2 * rows * TOPK // experts)
    group = EXP_DEV * most

    gate_t, up_t = jnp.swapaxes(expert_gate, 1, 2), jnp.swapaxes(expert_up, 1, 2)
    own_weights = jnp.concatenate([gate_t, up_t], axis=0).reshape(-1, width)
    weights = lax.all_gather(own_weights, "tp", axis=0)

    product = (in_gate.astype(f32) * conv_input.astype(f32)).astype(bf16)
    last = tokens - CONV_K + 1
    docs_row = jnp.broadcast_to(doc_ids[last:, None].astype(bf16), (CONV_K - 1, LANES))
    tail = jnp.concatenate([product[last:], docs_row], axis=1)
    before = lax.ppermute(tail, "sp", [(i, i + 1) for i in range(n_sp - 1)])
    extended = jnp.concatenate([before[:, :chans], product], axis=0).astype(f32)
    ext_docs = jnp.concatenate([before[:, chans].astype(jnp.int32), doc_ids])
    mixed = jnp.zeros(product_shape, f32)
    for k in range(CONV_K):
        keep = (ext_docs[k : k + tokens] == doc_ids)[:, None]
        mixed = mixed + jnp.where(keep, conv_taps[k] * extended[k : k + tokens], f32(0.0))
    conv_out = out_gate.astype(f32) * mixed
    conv_out = conv_out.astype(bf16)

    core = lax.axis_index("sp") % 2
    half = chans // 2
    scaled = (out_weight.astype(f32) * mix_gain[:, None]).astype(bf16)
    scaled = lax.dynamic_slice_in_dim(scaled, core * half, half, 0)
    scaled = jnp.moveaxis(scaled.reshape(half, n_tp, cols), 1, 0)
    gains = jnp.stack(split_bf16(ffn_gain, 3) + [jnp.zeros_like(ffn_gain)] * 5).astype(bf16)
    gains = jnp.broadcast_to(gains[None], (n_tp, *gains.shape))
    got = lax.all_to_all(jnp.concatenate([scaled, gains], axis=1), "tp", 0, 0, tiled=True)
    gain = got[:, half : half + 3].astype(f32)
    gain = ((gain[:, 0] + gain[:, 1]) + gain[:, 2]).reshape(1, width)
    here = got[:, :half]
    there = lax.ppermute(here, "sp", [(i, i + 1 - 2 * (i % 2)) for i in range(n_sp)])
    columns = jnp.concatenate(
        [jnp.where(core == 0, here, there), jnp.where(core == 0, there, here)], axis=1
    )

    copies = jnp.broadcast_to(conv_out[None], (n_tp, *conv_out.shape))
    channels = lax.all_to_all(copies, "tp", 0, 0, tiled=True)
    squares = jnp.sum(channels.astype(f32) * channels.astype(f32), axis=(0, 2))
    proj = lax.dot_general(
        jnp.moveaxis(channels, 0, 1).reshape(tokens, -1),
        columns.reshape(-1, cols),
        (((1,), (0,)), ((), ())),
        preferred_element_type=f32,
    )
    scale = lax.rsqrt(squares / (chans * n_tp) + EPS)[:, None]
    own = (residual.astype(f32) + proj * scale).astype(bf16)
    blocks = lax.all_to_all(own.reshape(n_tp, rows, cols), "tp", 0, 0, tiled=True)
    stream = jnp.moveaxis(blocks, 0, 1).reshape(rows, width)

    mine = lax.dynamic_slice_in_dim(routing, tp * rows, rows, 0).T
    slot = jnp.arange(experts * most, dtype=jnp.int32)[:, None]
    names = (mine[0:1] == slot // most) | (mine[1:2] == slot // most)
    order = jnp.arange(rows, dtype=jnp.int32)
    ahead = (order[:, None] < order[None, :]).astype(bf16)
    earlier = jnp.dot(names.astype(bf16), ahead, preferred_element_type=f32)
    pick = (names & (earlier == (slot % most).astype(f32))).astype(bf16)
    routed = jnp.dot(pick, stream, preferred_element_type=f32).astype(bf16)
    arrived = lax.all_to_all(routed.reshape(n_sp, most, EXP_DEV, width), "sp", 0, 0, tiled=True)

    hidden = hidden_of(arrived.reshape(n_sp * group, width), gain, weights, group, most)
    result = down_of(gather_near(hidden, "tp"), expert_down, group, most)
    returned = lax.all_to_all(result, "sp", 0, 0, tiled=True)

    everyone = lax.all_gather(stream, "tp", axis=0, tiled=True)
    everyone, _ = lax.optimization_barrier((everyone, result))
    every32 = everyone.astype(f32)
    mean = jnp.sum(every32 * every32, axis=1, keepdims=True) / width
    normal = (every32 * lax.rsqrt(mean + EPS) * gain).astype(bf16)
    last_dims = (((1,), (1,)), ((), ()))
    gate = lax.dot_general(shared_gate.T, normal, last_dims, preferred_element_type=f32)
    upper = lax.dot_general(shared_up.T, normal, last_dims, preferred_element_type=f32)
    shared_hid = (jax.nn.silu(gate) * upper).astype(bf16)

    hid_all = jnp.concatenate(gather_direct(shared_hid, "tp"), axis=0)
    own_first = jnp.concatenate([shared_down, shared_down], axis=0)
    own_first = lax.dynamic_slice_in_dim(
        own_first, tp * shared_hid.shape[0], shared_down.shape[0], 0
    )
    shared_part = lax.dot_general(
        hid_all, own_first, (((0,), (0,)), ((), ())), preferred_element_type=f32
    )

    token = jnp.arange(tokens, dtype=jnp.int32)
    all_names = (routing[:, :, None] == jnp.arange(experts, dtype=jnp.int32)).astype(bf16)
    before_it = (token[:, None] > token[None, :]) & (token[:, None] // rows == token[None, :] // rows)
    counts = jnp.dot(before_it.astype(bf16), all_names.sum(axis=1), preferred_element_type=f32)
    place = jnp.sum(counts[:, None, :] * all_names.astype(f32), axis=2).astype(jnp.int32)
    block = (token // rows - tp + n_tp) % n_tp
    entry = (
        routing // EXP_DEV * (n_tp * group)
        + block[:, None] * group
        + routing % EXP_DEV * most
        + place
    )
    at = jnp.arange(n_sp * n_tp * group, dtype=jnp.int32)[None, :]
    hits = [entry[:, k : k + 1] == at for k in range(TOPK)]
    picks = sum(jnp.where(hits[k], route_weight[:, k : k + 1], f32(0.0)) for k in range(TOPK))
    combined = jnp.dot(picks.astype(bf16), returned, preferred_element_type=f32)
    shared_part = own.astype(f32) + shared_part
    return (shared_part + combined).astype(bf16)


def solution(mesh):
    return jax.shard_map(
        body,
        mesh=mesh,
        in_specs=(
            P(("grp", "sp"), "tp"),
            P(("grp", "sp"), "tp"),
            P(("grp", "sp"), "tp"),
            P(("grp", "sp")),
            P(("grp", "sp"), "tp"),
            P(None, "tp"),
            P("tp"),
            P("tp", None),
            P("tp"),
            P(("grp", "sp"), None),
            P(("grp", "sp"), None),
            P("sp", None, "tp"),
            P("sp", None, "tp"),
            P("sp", None, "tp"),
            P(None, "tp"),
            P(None, "tp"),
            P(None, "tp"),
        ),
        out_specs=P(("grp", "sp"), "tp"),
        check_vma=False,
    )
```
